32 devices in a mesh: grp: 2 (over y), sp: 4 (over z), tp: 4 (over x, core).
Axes of the slice: x: 2, y: 2, z: 4, core: 2. Of those that a mesh axis runs over, the one named last changes fastest.
Arguments:
- queries: bfloat16 [4096, 2048], P(('grp', 'sp'), 'tp'), parts along dimension 0, may hold values from -64 to 64
- key_heads: bfloat16 [4096, 4, 64], P(('grp', 'sp'), 'tp'), parts along dimension 0, may hold values from -64 to 64
- value_heads: bfloat16 [4096, 4, 64], P(('grp', 'sp'), 'tp'), parts along dimension 0, may hold values from -6 to 6
- sink_logit: float32 [32], P('tp'), may hold values from 3 to 6
- out_weight: bfloat16 [2048, 2048], P('tp'), may hold values from -0.75 to 0.75
- residual: bfloat16 [4096, 2048], P(('grp', 'sp', 'tp')), parts along dimension 0, may hold values from -6 to 6
- norm_gain: float32 [2048], replicated, may hold values from 0.1 to 1.9
- expert_ids: int32 [4096, 2], P(('grp', 'sp', 'tp')), parts along dimension 0, may hold values from 0 to 15, all different within a row; in each aligned block of 128 rows (0 to 127, 128 to 255, ...) at most 32 rows name the same one
- route_weights: float32 [4096, 2], P(('grp', 'sp', 'tp')), parts along dimension 0, may hold values from 0.1 to 1
- gate_weight: bfloat16 [16, 2048, 512], P(('sp', 'tp')), may hold values from -0.125 to 0.125
- up_weight: bfloat16 [16, 2048, 512], P(('sp', 'tp')), may hold values from -0.125 to 0.125
- down_weight: bfloat16 [16, 512, 2048], P(('sp', 'tp')), may hold values from -0.5 to 0.5
Outputs:
- mixed: bfloat16 [4096, 2048], P(('grp', 'sp', 'tp')), parts along dimension 0
The draws below stay inside these ranges and needn't reach their ends.
There are 2 independent parts, one for each index of `grp`. The reference program is written for one: setup_inputs(seed, part) draws one part's arguments, and reference() takes and returns one part's arrays. A program takes and returns all parts, laid end to end along the dimension named above; an argument that names none is the same for every part. Nothing has to cross between parts.
Inputs may be any that keep to these rules, and one draw needn't show every extreme that they name: `expert_ids`: each row names 2 different experts. In the rows of one device (aligned blocks of 128 rows) no expert is named more than 32 times, and in some blocks one expert is named exactly 32 times.
All inputs are finite; a program needn't handle non-finite values.
Results may differ from the reference program's by a relative error of at most 0.014.
Values may be sent and summed in bfloat16 or wider, within the bound.
A program may use at most 64 MiB of HBM per device.

```python
import math
import jax
import jax.numpy as jnp
import numpy as np
from jax import lax

D = 2048
QH = 32
KVH = 4
HEAD_SIZE = 64
WINDOW = 128
FF = 512
TOP_K = 2
TOK_DEV = 128
TOKENS = 2048
EXPERTS = 16
CAP = 32


def draw_queries(key, part):
    drawn = jnp.clip(jax.random.normal(jax.random.fold_in(key, 5), (TOKENS, QH * HEAD_SIZE), jnp.float32), -6.0, 6.0)
    return drawn.astype(jnp.bfloat16)


def draw_key_heads(key, part):
    drawn = jnp.clip(jax.random.normal(jax.random.fold_in(key, 6), (TOKENS, KVH, HEAD_SIZE), jnp.float32), -6.0, 6.0)
    return drawn.astype(jnp.bfloat16)


def steps_of(own_key, dims, pieces, least, largest):
    level, own = 1.0, jax.random.fold_in(own_key, 6)
    for position, parts in pieces:
        steps = jnp.exp(jax.random.uniform(jax.random.fold_in(own, position), (parts,), jnp.float32, least / len(pieces), largest / len(pieces)))
        level = level * jnp.repeat(steps, dims[position] // parts).reshape([-1 if axis == position else 1 for axis in range(len(dims))])
    return level


def assign_block(own_key, own, number, rows, amount, top, limit, lean):
    ranking = jax.random.permutation(own_key, amount)
    crowded, ordinary = portions_of(amount, rows * top, limit, lean, True), portions_of(amount, rows * top, limit, lean, False)
    places = jnp.arange(amount)

    def named(sizes, turn):
        used = int((sizes > 0).sum())
        fixed = max(1, used // 4)
        shifted = fixed + (places - fixed + turn * (used - fixed)) % max(1, amount - fixed)
        return jnp.zeros((amount,), jnp.int32).at[ranking[jnp.where(places < fixed, places, shifted)]].set(jnp.asarray(sizes, jnp.int32))

    sizes = jnp.where(number % 4 == 0, named(crowded, number // 4), named(ordinary, number - number // 4 - 1))
    mixed = jax.random.permutation(jax.random.fold_in(own, 3), amount)
    giver, receiver = mixed[0:amount // 2 * 2:2], mixed[1:amount // 2 * 2:2]
    room = jnp.minimum(sizes[giver] - 1, limit - sizes[receiver]) // 2
    room = jnp.where((giver == ranking[0]) | (receiver == ranking[0]) | (sizes[receiver] == 0), 0, jnp.maximum(room, 0))
    shifted = jax.random.randint(jax.random.fold_in(own, 4), (amount // 2,), 0, 1 << 20) % (room + 1)
    sizes = sizes.at[giver].add(-shifted).at[receiver].add(shifted)
    members = jnp.searchsorted(jnp.cumsum(sizes), jnp.arange(rows * top), side="right").astype(jnp.int32)
    table = members.reshape(top, rows).T
    table = table[jax.random.permutation(jax.random.fold_in(own, 1), rows)]
    turn = jax.random.randint(jax.random.fold_in(own, 2), (rows, 1), 0, top)
    return jnp.take_along_axis(table, (jnp.arange(top)[None, :] + turn) % top, axis=1)


def portions_of(amount, total, limit, skew, full):
    loads = [(1 << 20) // math.isqrt(grade ** skew) + 1 for grade in range(1, amount + 1)]
    largest = limit if full else min(limit, max(-(-total // amount), total * loads[0] // sum(loads)))
    least = 1 if total - largest >= amount - 1 else 0
    holding, rest = [largest] + [least] * (amount - 1), total - largest - least * (amount - 1)
    while rest > 0:
        free = [i for i in range(1, amount) if holding[i] < largest] or [i for i in range(1, amount) if holding[i] < limit]
        whole, left = sum([loads[i] for i in free]), rest
        for i in free:
            extra = min(limit - holding[i], max(1, left * loads[i] // whole), rest)
            holding[i] = holding[i] + extra
            rest = rest - extra
    return np.array(holding)


def normal_values(rng, dims, deviation, limit, pieces=(), kind=jnp.bfloat16):
    gain = steps_of(rng, dims, pieces, -0.22, 0.18) if pieces else 1.0
    result = jax.random.normal(rng, dims, jnp.float32) * deviation * gain
    return jnp.minimum(jnp.maximum(result, -limit), limit).astype(kind)


def setup_inputs(seed: int = 0, part: int = 0) -> dict:
    key_list = jax.random.split(jax.random.key(seed), 13)
    own_keys = jax.random.split(jax.random.fold_in(key_list[12], part), 13)
    queries = draw_queries(jax.random.fold_in(jax.random.fold_in(key_list[12], part), 71), part)
    key_heads = draw_key_heads(jax.random.fold_in(jax.random.fold_in(key_list[12], part), 71), part)
    value_heads = normal_values(own_keys[2], (TOKENS, KVH, HEAD_SIZE), 1.0, 6.0, ((0, 4), (1, 4)))
    sink_logit = jnp.clip(3.0 + 3.0 * jax.random.uniform(key_list[3], (QH,), jnp.float32) ** steps_of(key_list[3], (QH,), ((0, 4),), -0.2, 0.2), 3.0, 6.0)
    out_weight = normal_values(key_list[4], (QH * HEAD_SIZE, D), (QH * HEAD_SIZE // 32) ** -0.5, 0.75, ((0, 4),))
    residual = normal_values(own_keys[5], (TOKENS, D), 1.0, 6.0, ((0, 16),))
    norm_gain = jnp.clip(1.0 + 0.18 * jax.random.normal(key_list[6], (D,), jnp.float32), 0.1, 1.9)
    expert_ids_keys = jax.random.split(jax.random.fold_in(own_keys[7], 1), TOKENS // TOK_DEV)
    expert_ids_turns = jax.random.permutation(jax.random.fold_in(own_keys[7], 3), TOKENS // TOK_DEV)
    expert_ids = jax.vmap(lambda own, number: assign_block(jax.random.fold_in(own_keys[7], 2), own, number, TOK_DEV, EXPERTS, TOP_K, CAP, 1))(expert_ids_keys, expert_ids_turns).reshape((TOKENS, TOP_K))
    route_weights = jnp.clip(jnp.exp(math.log(1.0) - 2.3025851 * jax.random.uniform(own_keys[8], (TOKENS, TOP_K), jnp.float32) ** steps_of(own_keys[8], (TOKENS, TOP_K), ((0, 16),), -0.2, 0.2)), 0.1, 1.0)
    gate_weight = normal_values(key_list[9], (EXPERTS, D, FF), D ** -0.5, 0.125, ((0, 16),))
    up_weight = normal_values(key_list[10], (EXPERTS, D, FF), D ** -0.5, 0.125, ((0, 16),))
    down_weight = normal_values(key_list[11], (EXPERTS, FF, D), (FF // 4) ** -0.5, 0.5, ((0, 16),))
    return dict(queries=queries, key_heads=key_heads, value_heads=value_heads, sink_logit=sink_logit, out_weight=out_weight, residual=residual, norm_gain=norm_gain, expert_ids=expert_ids, route_weights=route_weights, gate_weight=gate_weight, up_weight=up_weight, down_weight=down_weight)


EPS = 1e-06

def attention(queries, key_heads, value_heads, sink_logit):
    group_size = QH // KVH
    count_of_blocks = TOKENS // WINDOW
    query_blocks = queries.reshape(count_of_blocks, WINDOW, KVH, group_size, HEAD_SIZE)
    key_blocks = key_heads.reshape(count_of_blocks, WINDOW, KVH, HEAD_SIZE)
    value_blocks = value_heads.reshape(count_of_blocks, WINDOW, KVH, HEAD_SIZE)
    blank = jnp.zeros((1, WINDOW, KVH, HEAD_SIZE), key_heads.dtype)
    key_span = jnp.concatenate([jnp.concatenate([blank, key_blocks[:-1]], 0), key_blocks], 1)
    value_span = jnp.concatenate([jnp.concatenate([blank, value_blocks[:-1]], 0), value_blocks], 1)
    query_pos = jnp.arange(WINDOW, dtype=jnp.int32)[:, None]
    key_pos = jnp.arange(2 * WINDOW, dtype=jnp.int32)[None, :]
    distance = query_pos + WINDOW - key_pos
    band = (distance >= 0) & (distance < WINDOW)
    key_start = jnp.arange(count_of_blocks, dtype=jnp.int32)[:, None] * WINDOW - WINDOW + key_pos
    allowed = band[None, :, :] & (key_start >= 0)[:, None, :]
    sinks = sink_logit.reshape(KVH, group_size)

    def one_head(packed):
        query_per_head, key_per_head, value_per_head, head_sink = packed
        logit_scores = jnp.einsum('szue,sje->suzj', query_per_head.astype(jnp.float32), key_per_head.astype(jnp.float32)) * HEAD_SIZE ** (-0.5)
        logit_scores = jnp.where(allowed[:, None], logit_scores, -jnp.inf)
        sink_col = head_sink[None, :, None, None]
        row_max = jnp.maximum(lax.optimization_barrier(jnp.max(logit_scores, axis=-1, keepdims=True)), sink_col)
        expd = jnp.exp(logit_scores - row_max)
        row_total = lax.optimization_barrier(jnp.sum(expd, axis=-1, keepdims=True)) + jnp.exp(sink_col - row_max)
        attention_probabilities = (expd / row_total).astype(jnp.bfloat16)
        return jnp.einsum('vjwu,vuo->vwjo', attention_probabilities.astype(jnp.float32), value_per_head.astype(jnp.float32)).astype(jnp.bfloat16)
    outputs = lax.map(one_head, (jnp.moveaxis(query_blocks, 2, 0), jnp.moveaxis(key_span, 2, 0), jnp.moveaxis(value_span, 2, 0), sinks))
    return jnp.moveaxis(outputs, 0, 2).reshape(TOKENS, QH * HEAD_SIZE)

def reference(queries, key_heads, value_heads, sink_logit, out_weight, residual, norm_gain, expert_ids, route_weights, gate_weight, up_weight, down_weight):
    attended = attention(queries, key_heads, value_heads, sink_logit)
    projected = jnp.dot(attended, out_weight, preferred_element_type=jnp.float32)
    stream = (residual.astype(jnp.float32) + projected).astype(jnp.bfloat16)
    wide = stream.astype(jnp.float32)
    normed = (wide * lax.rsqrt(lax.optimization_barrier(jnp.mean(wide * wide, axis=-1, keepdims=True)) + EPS) * norm_gain).astype(jnp.bfloat16)
    device_count = TOKENS // TOK_DEV
    pairs = TOK_DEV * TOP_K
    flat_ids = expert_ids.reshape(device_count, pairs)
    onehot = (flat_ids[:, :, None] == jnp.arange(EXPERTS, dtype=jnp.int32)[None, None, :]).astype(jnp.int32)
    earlier = jnp.cumsum(onehot, axis=1) - onehot
    slot_rank = lax.optimization_barrier(jnp.sum(earlier * onehot, axis=-1))
    flat_slot = (flat_ids * CAP + slot_rank).astype(jnp.int32)
    device_row = jnp.arange(device_count, dtype=jnp.int32)[:, None]
    owner_row = device_row * TOK_DEV + (jnp.arange(pairs, dtype=jnp.int32) // TOP_K)[None, :]
    shares = route_weights / lax.optimization_barrier(jnp.sum(route_weights, axis=-1, keepdims=True))
    token_in_slot = jnp.zeros((device_count, EXPERTS * CAP), jnp.int32).at[device_row, flat_slot].set(owner_row)
    slot_share = jnp.zeros((device_count, EXPERTS * CAP), jnp.float32).at[device_row, flat_slot].set(shares.reshape(device_count, pairs))

    def expert_step(summed, packed):
        w_gate_e, w_up_e, w_down_e, expert = packed
        row_index = lax.dynamic_slice_in_dim(token_in_slot, expert * CAP, CAP, 1).reshape(-1)
        row_share = lax.dynamic_slice_in_dim(slot_share, expert * CAP, CAP, 1).reshape(-1)
        rows = normed[row_index]
        gate = jnp.dot(rows, w_gate_e, preferred_element_type=jnp.float32)
        upward = jnp.dot(rows, w_up_e, preferred_element_type=jnp.float32)
        expert_hidden = (jax.nn.silu(gate) * upward).astype(jnp.bfloat16)
        expert_rows = jnp.dot(expert_hidden, w_down_e, preferred_element_type=jnp.float32).astype(jnp.bfloat16)
        summed = summed.at[row_index].add(row_share[:, None] * expert_rows.astype(jnp.float32))
        return (summed, None)
    start = jnp.zeros((TOKENS, D), jnp.float32)
    summed, _ = lax.scan(expert_step, start, (gate_weight, up_weight, down_weight, jnp.arange(EXPERTS, dtype=jnp.int32)))
    return (stream.astype(jnp.float32) + summed).astype(jnp.bfloat16)
```

```python
import functools

import jax
import jax.numpy as jnp
from jax import lax
from jax.experimental import pallas as pl
from jax.experimental.pallas import tpu as pltpu
from jax.sharding import PartitionSpec as P

WINDOW = 128


EPS = 1e-06

F32 = jnp.float32
BF16 = jnp.bfloat16
MESH = pl.DeviceIdType.MESH
VMEM_BUDGET = 56 * 1024 * 1024


def from_behind(value, axis, steps):
    count = lax.axis_size(axis)
    initial, last = (max(0, -steps), min(count, count - steps))
    return lax.ppermute(value, axis, [(source, source + steps) for source in range(initial, last)])


def dot(a, b, dims=((1,), (0,))):
    return lax.dot_general(a, b, (dims, ((), ())), preferred_element_type=F32)


def attention(queries, key_heads, value_heads, sink_logit):
    rows_sp = queries.shape[0]
    kv_local = key_heads.shape[1]
    head_dim = key_heads.shape[2]
    heads_local = queries.shape[1] // head_dim
    group_size = heads_local // kv_local
    window = WINDOW
    count_of_blocks = rows_sp // window
    edge = jnp.stack([key_heads[rows_sp - window :], value_heads[rows_sp - window :]])
    tail_rows = from_behind(edge, "sp", 1)
    key_blocks = jnp.concatenate([tail_rows[0], key_heads], 0).reshape(
        count_of_blocks + 1, window, kv_local, head_dim
    )
    value_blocks = jnp.concatenate([tail_rows[1], value_heads], 0).reshape(
        count_of_blocks + 1, window, kv_local, head_dim
    )
    key_span = jnp.concatenate([key_blocks[:-1], key_blocks[1:]], 1)
    value_span = jnp.concatenate([value_blocks[:-1], value_blocks[1:]], 1)
    query_pos = jnp.arange(window, dtype=jnp.int32)[:, None]
    key_pos = jnp.arange(2 * window, dtype=jnp.int32)[None, :]
    distance = query_pos + window - key_pos
    band = (distance >= 0) & (distance < window)
    key_start = (
        lax.axis_index("sp") * rows_sp
        + jnp.arange(count_of_blocks, dtype=jnp.int32)[:, None] * window
        - window
        + key_pos
    )
    allowed = band[None, :, :] & (key_start >= 0)[:, None, :]
    query_blocks = queries.reshape(count_of_blocks, window, kv_local, group_size, head_dim)
    logit_scores = jnp.einsum(
        "bqhgd,bkhd->bhgqk", query_blocks, key_span, preferred_element_type=jnp.float32
    ) * head_dim ** (-0.5)
    logit_scores = jnp.where(allowed[:, None, None], logit_scores, -jnp.inf)
    sink_col = sink_logit.reshape(kv_local, group_size)[None, :, :, None, None]
    row_max = jnp.maximum(jnp.max(logit_scores, axis=-1, keepdims=True), sink_col)
    expd = jnp.exp(logit_scores - row_max)
    row_total = jnp.sum(expd, axis=-1, keepdims=True) + jnp.exp(sink_col - row_max)
    attention_probabilities = (expd / row_total).astype(jnp.bfloat16)
    attended = jnp.einsum(
        "bhgqk,bkhd->bqhgd", attention_probabilities, value_span, preferred_element_type=jnp.float32
    ).astype(jnp.bfloat16)
    return attended.reshape(rows_sp, heads_local * head_dim)


def tail_plain(
    attended, out_weight, residual, norm_gain, expert_ids, route_weights,
    gate_weight, up_weight, down_weight,
):
    rows_dev = residual.shape[0]
    width = residual.shape[1]
    projected = lax.psum_scatter(
        jnp.dot(attended, out_weight, preferred_element_type=jnp.float32),
        "tp",
        scatter_dimension=0,
        tiled=True,
    )
    stream = (residual.astype(jnp.float32) + projected).astype(jnp.bfloat16)
    wide = stream.astype(jnp.float32)
    normed = (
        wide * lax.rsqrt(jnp.mean(wide * wide, axis=-1, keepdims=True) + EPS) * norm_gain
    ).astype(jnp.bfloat16)
    sp_count = lax.axis_size("sp")
    tp_count = lax.axis_size("tp")
    experts_total = sp_count * tp_count
    top_k = expert_ids.shape[1]
    capacity = max(2, 2 * top_k * rows_dev // experts_total)
    flat_ids = expert_ids.reshape(-1)
    pairs = flat_ids.shape[0]
    onehot = (flat_ids[:, None] == jnp.arange(experts_total, dtype=jnp.int32)[None, :]).astype(
        jnp.int32
    )
    earlier = jnp.cumsum(onehot, axis=0) - onehot
    slot_rank = jnp.sum(earlier * onehot, axis=1)
    flat_slot = flat_ids * capacity + slot_rank
    owner_row = jnp.arange(pairs, dtype=jnp.int32) // top_k
    token_in_slot = jnp.zeros((experts_total * capacity,), jnp.int32).at[flat_slot].set(owner_row)
    filled = jnp.zeros((experts_total * capacity,), jnp.bool_).at[flat_slot].set(True)
    outbox = jnp.where(filled[:, None], normed[token_in_slot], jnp.zeros((), jnp.bfloat16))
    outbox = outbox.reshape(experts_total, capacity, width)
    arrived = lax.all_to_all(outbox, ("sp", "tp"), split_axis=0, concat_axis=0, tiled=True)
    rows = arrived.reshape(-1, width)
    gate = jnp.dot(rows, gate_weight[0], preferred_element_type=jnp.float32)
    upward = jnp.dot(rows, up_weight[0], preferred_element_type=jnp.float32)
    expert_hidden = (jax.nn.silu(gate) * upward).astype(jnp.bfloat16)
    expert_rows = jnp.dot(expert_hidden, down_weight[0], preferred_element_type=jnp.float32).astype(
        jnp.bfloat16
    )
    results = expert_rows.reshape(arrived.shape)
    returned = lax.all_to_all(results, ("sp", "tp"), split_axis=0, concat_axis=0, tiled=True)
    picked_rows = returned.reshape(experts_total * capacity, width)[flat_slot].reshape(
        rows_dev, top_k, width
    )
    shares = route_weights / jnp.sum(route_weights, axis=-1, keepdims=True)
    combined = jnp.sum(shares[:, :, None] * picked_rows.astype(jnp.float32), axis=1)
    return (wide + combined).astype(jnp.bfloat16)


def routing(facts, first, top_k, experts, capacity):
    facts = facts.T
    rows = facts.shape[0]
    ids, weights = facts[:, :top_k], facts[:, top_k : 2 * top_k]
    expert = (first + lax.broadcasted_iota(jnp.int32, (rows, experts), 1)).astype(F32)
    total = jnp.sum(weights, axis=1, keepdims=True)
    member = jnp.zeros((rows, experts), F32)
    share = jnp.zeros((rows, experts), F32)
    for k in range(top_k):
        hit = jnp.where(ids[:, k : k + 1] == expert, 1.0, 0.0)
        member = member + hit
        share = share + hit * (weights[:, k : k + 1] / total)
    before = (
        lax.broadcasted_iota(jnp.int32, (rows, rows), 0)
        > lax.broadcasted_iota(jnp.int32, (rows, rows), 1)
    ).astype(BF16)
    rank = dot(before, member.astype(BF16))
    rank = jnp.where(member > 0, rank, -1.0)
    slots = experts * capacity
    spread = (
        lax.broadcasted_iota(jnp.int32, (experts, slots), 1) // capacity
        == lax.broadcasted_iota(jnp.int32, (experts, slots), 0)
    ).astype(BF16)
    rank_slot = dot(rank.astype(BF16), spread)
    place = lax.broadcasted_iota(jnp.int32, (rows, slots), 1) % capacity
    taken = rank_slot == place.astype(F32)
    high = share.astype(BF16)
    low = (share - high.astype(F32)).astype(BF16)
    one = jnp.where(taken, 1.0, 0.0)
    shares = jnp.concatenate([one * dot(high, spread), one * dot(low, spread)], 0)
    return one.T.astype(BF16), shares.astype(BF16)


def attend(z, token_rows, queries, sink, seen, attended, at):
    window = WINDOW
    rows, lanes = queries.shape[0], seen.shape[1]
    heads = sink.shape[1]
    size = queries.shape[1] // heads
    groups = lanes // (2 * size)
    share = heads // groups
    pairs = share // 2
    tall = pairs * window
    query = lax.broadcasted_iota(jnp.int32, (tall, 2 * window), 0) % window
    key = lax.broadcasted_iota(jnp.int32, (tall, 2 * window), 1)
    distance = query + window - key
    band = (distance >= 0) & (distance < window)

    def block(b):
        allowed = band & ((z * rows + b * window - window) + key >= 0)
        span = seen[pl.ds(pl.multiple_of(b * window, window), 2 * window), :]
        here = pl.ds(pl.multiple_of(b * window, window), window)
        for g in range(groups):
            keys = span[:, 2 * g * size : (2 * g + 1) * size]
            values = span[:, (2 * g + 1) * size : (2 * g + 2) * size]
            none, ones = jnp.zeros_like(keys), jnp.ones_like(values)
            wide = jnp.concatenate(
                [
                    queries[here, (g * share + 2 * i) * size : (g * share + 2 * i + 2) * size]
                    for i in range(pairs)
                ],
                0,
            )
            sides = []
            for odd in range(2):
                two_keys = jnp.concatenate([none, keys] if odd else [keys, none], 1)
                two_values = jnp.concatenate([ones, values] if odd else [values, ones], 1)
                score = dot(wide, two_keys, ((1,), (1,))) * size**-0.5
                score = jnp.where(allowed, score, -1e30)
                drain = jnp.concatenate(
                    [
                        jnp.broadcast_to(
                            sink[0:1, g * share + 2 * i + odd : g * share + 2 * i + odd + 1],
                            (window, 1),
                        )
                        for i in range(pairs)
                    ],
                    0,
                )
                top = jnp.maximum(jnp.max(score, axis=1, keepdims=True), drain)
                grown = jnp.exp(score - top).astype(BF16)
                both = dot(grown, two_values)
                at = 0 if odd else size
                total = both[:, at : at + 1] + jnp.exp(drain - top)
                sides.append(both * (1.0 / total))
            lane = lax.broadcasted_iota(jnp.int32, (tall, 2 * size), 1)
            both = jnp.where(lane < size, sides[0], sides[1]).astype(BF16)
            for i in range(pairs):
                first = (g * share + 2 * i) * size
                attended[here, first : first + 2 * size] = both[i * window : (i + 1) * window]

    for b in range(token_rows // window):
        block(at * (token_rows // window) + b)


def plan(m, count, pieces):
    piece, hop = 1.0 / pieces, 0.15
    exchange = 0.65
    mix = 1.25

    def due(s):
        return abs(s - m)

    steps = []
    for s in range(count):
        for q in range(pieces):
            at = 0.0 if s == m else due(s) - 1 + (q + 1) * piece + hop
            steps.append((at, "pick", s, q))
        steps.append((due(s) + exchange, "expert", s, 0))
        steps.append((due(s) + mix, "mix", s, 0))
        if s != m and m > 0:
            origin = 0 if s > m else count - 1
            for q in range(pieces):
                at = abs(s - origin) + mix + abs(m - origin) * 0.35 + q * piece
                steps.append((max(at, due(s) + mix + 0.01), "pass", s, q))
    steps.sort(key=lambda step: step[0])
    return [step[1:] for step in steps]


def tail_kernel(
    sizes,
    queries, kv, sink, out_w_hbm, residual, gain, ids, weights, gate_hbm, up_hbm, down_hbm,
    out,
    seen, attended, halo_send, halo_recv,
    out_w, gate_w, up_w, down_w,
    pair_out, pair_in, far_out, far_in,
    stream, facts, slots, shares,
    tokens, outbox, arrived, results, returned,
    local, total_own, line_out, line_in,
    load_sem, pair_send, pair_recv, far_send, far_recv,
    facts_send, facts_recv, line_go_send, line_go_recv,
    go_send, go_recv, back_send, back_recv, line_back_send, line_back_recv,
):
    sp_count, tp_count, pieces, capacity = sizes
    chips = tp_count // 2
    z, t = lax.axis_index("sp"), lax.axis_index("tp")
    x, core = t // 2, t % 2
    other = 1 - core
    rows, width = residual.shape
    piece = width // pieces
    top_k = ids.shape[0]
    picks = tp_count * capacity

    loads = [
        pltpu.make_async_copy(src, dst, load_sem.at[i])
        for i, (src, dst) in enumerate(
            ((out_w_hbm, out_w), (gate_hbm.at[0], gate_w), (up_hbm.at[0], up_w), (down_hbm.at[0], down_w))
        )
    ]
    for load in loads:
        load.start()

    barrier = pltpu.get_barrier_semaphore()
    for k in range(1, sp_count):
        pl.semaphore_signal(
            barrier, inc=1, device_id={"sp": (z + k) % sp_count}, device_id_type=MESH
        )
    for k in range(1, tp_count):
        pl.semaphore_signal(
            barrier, inc=1, device_id={"tp": (t + k) % tp_count}, device_id_type=MESH
        )
    pl.semaphore_wait(barrier, sp_count + tp_count - 2)
    reach = kv.shape[0]
    halo_copy = pltpu.make_async_remote_copy(
        kv.at[pl.ds(reach - WINDOW, WINDOW)], seen.at[pl.ds(0, WINDOW)], halo_send, halo_recv,
        device_id={"sp": jnp.minimum(z + 1, sp_count - 1)}, device_id_type=MESH,
    )

    @pl.when(z < sp_count - 1)
    def _():
        halo_copy.start()

    def facts_copy(k):
        return pltpu.make_async_remote_copy(
            facts.at[z], facts.at[z], facts_send.at[k], facts_recv.at[z],
            device_id={"sp": (z + k) % sp_count}, device_id_type=MESH,
        )

    def facts_wait(s):
        pltpu.make_async_remote_copy(
            facts.at[s], facts.at[s], facts_send.at[0], facts_recv.at[s],
            device_id={"sp": s}, device_id_type=MESH,
        ).wait_recv()

    pad = jnp.zeros((-2 * top_k % 8, rows), F32)
    facts[z] = jnp.concatenate([ids[...].astype(F32), weights[...], pad], 0)
    for k in range(1, sp_count):
        facts_copy(k).start()

    seen[WINDOW:, :] = kv[...]

    def route(s):
        slots[s], shares[s] = routing(facts[s], z * tp_count, top_k, tp_count, capacity)

    @pl.when(z == 0)
    def _():
        seen[:WINDOW, :] = jnp.zeros((WINDOW, kv.shape[1]), BF16)

    @pl.when(z > 0)
    def _():
        halo_copy.wait_recv()

    loads[0].wait()

    def partial(chip, which, q):
        block = attended[pl.ds(pl.multiple_of((chip * 2 + which) * rows, rows), rows), :]
        return dot(block, out_w[:, q * piece : (q + 1) * piece])

    def pair_copy(k, q):
        return pltpu.make_async_remote_copy(
            pair_out.at[k, q], pair_in.at[k, q], pair_send.at[k, q], pair_recv.at[k, q],
            device_id={"tp": x * 2 + other}, device_id_type=MESH,
        )

    def far_copy(k, q):
        return pltpu.make_async_remote_copy(
            far_out.at[k, q], far_in.at[k, q], far_send.at[k, q], far_recv.at[k, q],
            device_id={"tp": ((x + k) % chips) * 2 + core}, device_id_type=MESH,
        )

    order = list(range(1, chips)) + [0]
    for k in order:
        chip = (x + k) % chips
        attend(z, rows, queries, sink, seen, attended, chip * 2 + other)
        for q in range(pieces):
            pair_out[k, q] = partial(chip, other, q).astype(BF16)
            pair_copy(k, q).start()
        attend(z, rows, queries, sink, seen, attended, chip * 2 + core)
        for q in range(pieces if k else 0):
            mine = partial(chip, core, q)
            pair_copy(k, q).wait_recv()
            far_out[k, q] = (mine + pair_in[k, q].astype(F32)).astype(BF16)
            far_copy(k, q).start()

    def route_other(k, carry):
        s = (z + k) % sp_count
        facts_wait(s)
        route(s)
        return carry

    route(z)
    lax.fori_loop(1, sp_count, route_other, 0)
    square = jnp.zeros((rows, 1), F32)
    for q in range(pieces):
        cols = slice(q * piece, (q + 1) * piece)
        total = partial(x, core, q)
        pair_copy(0, q).wait_recv()
        total = total + pair_in[0, q].astype(F32)
        for k in range(1, chips):
            far_copy(k, q).wait_recv()
            total = total + far_in[k, q].astype(F32)
        value = (residual[:, cols].astype(F32) + total).astype(BF16)
        stream[:, cols] = value
        value = value.astype(F32)
        square = square + jnp.sum(value * value, axis=1, keepdims=True)
    scale = lax.rsqrt(square / width + EPS)

    def line_go(to, s, q, way):
        return pltpu.make_async_remote_copy(
            tokens.at[s, q], tokens.at[s, q], line_go_send.at[way, s, q], line_go_recv.at[s, q],
            device_id={"sp": to}, device_id_type=MESH,
        )

    def line_back(to, s, q, way):
        return pltpu.make_async_remote_copy(
            line_out.at[s, q], line_in.at[way, s, q], line_back_send.at[s, q],
            line_back_recv.at[way, s, q], device_id={"sp": to}, device_id_type=MESH,
        )

    def go_copy(s, q, to, at):
        return pltpu.make_async_remote_copy(
            outbox.at[s, q, to], arrived.at[s, q, at], go_send.at[s, q, to], go_recv.at[s, q, at],
            device_id={"tp": to}, device_id_type=MESH,
        )

    def back_copy(s, q, to, at):
        return pltpu.make_async_remote_copy(
            results.at[s, q, to], returned.at[s, q, at], back_send.at[s, q, to], back_recv.at[s, q, at],
            device_id={"tp": to}, device_id_type=MESH,
        )

    peers = [(t + k) % tp_count for k in range(1, tp_count)]
    flip = (z * 2 >= sp_count).astype(jnp.int32)
    place = z + flip * (sp_count - 1 - 2 * z)

    def real(s):
        return s + flip * (sp_count - 1 - 2 * s)

    def program(m):
        inner, outer = flip, 1 - flip

        def pick(s, q):
            r = real(s)
            if s == m:
                cols = slice(q * piece, (q + 1) * piece)
                tokens[r, q] = (stream[:, cols].astype(F32) * scale * gain[:, cols]).astype(BF16)
                line_go(real(m + 1), r, q, inner).start()
                if m > 0:
                    line_go(real(m - 1), r, q, outer).start()
            else:
                line_go(r, r, q, inner).wait_recv()
                if s < m:
                    line_go(real(m + 1), r, q, inner).start()
                elif m > 0:
                    line_go(real(m - 1), r, q, outer).start()
            chosen = dot(slots[r], tokens[r, q]).astype(BF16)
            outbox[r, q] = chosen.reshape(tp_count, capacity, piece)
            for to in peers:
                go_copy(r, q, to, t).start()
            arrived[r, q, t] = outbox[r, q, t]

        def expert(s, _):
            r = real(s)
            gated = raised = None
            for q in range(pieces):
                for peer in peers:
                    go_copy(r, q, peer, peer).wait_recv()
                block = arrived[r, q].reshape(picks, piece)
                part = slice(q * piece, (q + 1) * piece)
                a, b = dot(block, gate_w[part, :]), dot(block, up_w[part, :])
                gated, raised = (a, b) if q == 0 else (gated + a, raised + b)
            hidden = (gated / (1.0 + jnp.exp(-gated)) * raised).astype(BF16)
            for q in range(pieces):
                done = dot(hidden, down_w[:, q * piece : (q + 1) * piece]).astype(BF16)
                results[r, q] = done.reshape(tp_count, capacity, piece)
                for to in peers:
                    back_copy(r, q, to, t).start()
                returned[r, q, t] = results[r, q, t]

        def mix(s, _):
            r = real(s)
            for q in range(pieces):
                for peer in peers:
                    back_copy(r, q, peer, peer).wait_recv()
                both = dot(shares[r], returned[r, q].reshape(picks, piece))
                mixed = both[:rows] + both[rows:]
                if s == m:
                    total_own[q] = stream[:, q * piece : (q + 1) * piece].astype(F32) + mixed
                elif m == 0:
                    line_out[r, q] = mixed.astype(BF16)
                    line_back(real(1), r, q, inner).start()
                else:
                    local[r, q] = mixed

        def hand_on(s, q):
            r = real(s)
            way, to = (inner, m + 1) if s > m else (outer, m - 1)
            line_back(real(to), r, q, way).wait_recv()
            line_out[r, q] = (local[r, q] + line_in[way, r, q].astype(F32)).astype(BF16)
            line_back(real(to), r, q, way).start()

        act = {"pick": pick, "expert": expert, "mix": mix, "pass": hand_on}
        loaded = False
        for name, s, q in plan(m, sp_count, pieces):
            if name == "expert" and not loaded:
                loaded = True
                for load in loads[1:]:
                    load.wait()
            act[name](s, q)
        for q in range(pieces):
            total = total_own[q]
            for way in [inner, outer] if m > 0 else [outer]:
                line_back(real(m + 1), z, q, way).wait_recv()
                total = total + line_in[way, z, q].astype(F32)
            out[:, q * piece : (q + 1) * piece] = total.astype(BF16)
        for s in range(sp_count):
            for q in range(pieces):
                r = real(s)
                if s <= m:
                    line_go(real(m + 1), r, q, inner).wait_send()
                if s >= m and m > 0:
                    line_go(real(m - 1), r, q, outer).wait_send()
                if s != m:
                    line_back(real(m + 1), r, q, inner).wait_send()

    for m in range((sp_count + 1) // 2):
        pl.when(place == m)(functools.partial(program, m))

    @pl.when(z < sp_count - 1)
    def _():
        halo_copy.wait_send()

    for k in range(1, sp_count):
        facts_copy(k).wait_send()
    for q in range(pieces):
        for k in range(chips):
            pair_copy(k, q).wait_send()
            if k:
                far_copy(k, q).wait_send()

    def flush(i, carry):
        s, q = i // pieces, i % pieces
        for peer in peers:
            go_copy(s, q, peer, t).wait_send()
            back_copy(s, q, peer, t).wait_send()
        return carry

    lax.fori_loop(0, sp_count * pieces, flush, 0)


def fused(
    queries, key_heads, value_heads, sink_logit, out_weight, residual, norm_gain, expert_ids, route_weights,
    gate_weight, up_weight, down_weight,
):
    rows, width = residual.shape
    sp_count, tp_count = lax.axis_size("sp"), lax.axis_size("tp")
    experts = sp_count * tp_count
    top_k = expert_ids.shape[1]
    capacity = max(2, 2 * top_k * rows // experts)
    hidden = gate_weight.shape[2]
    depth = out_weight.shape[0]
    pieces = 4
    chips = tp_count // 2
    piece = width // pieces
    part = (chips, pieces, rows, piece)
    line = (sp_count, pieces, rows, piece)
    box = (sp_count, pieces, tp_count, capacity, piece)
    picks = tp_count * capacity
    reach, groups, size = key_heads.shape
    kv = jnp.stack([key_heads, value_heads], 2).reshape(reach, groups * 2 * size)
    vmem = pl.BlockSpec(memory_space=pltpu.VMEM)
    hbm = pl.BlockSpec(memory_space=pl.ANY)
    dma = pltpu.SemaphoreType.DMA
    return pl.pallas_call(
        functools.partial(tail_kernel, (sp_count, tp_count, pieces, capacity)),
        out_shape=jax.ShapeDtypeStruct((rows, width), BF16),
        in_specs=[vmem, vmem, vmem, hbm, vmem, vmem, vmem, vmem, hbm, hbm, hbm],
        out_specs=vmem,
        scratch_shapes=[
            pltpu.VMEM((WINDOW + kv.shape[0], kv.shape[1]), BF16),
            pltpu.VMEM(queries.shape, BF16),
            dma,
            dma,
            pltpu.VMEM((depth, width), BF16),
            pltpu.VMEM((width, hidden), BF16),
            pltpu.VMEM((width, hidden), BF16),
            pltpu.VMEM((hidden, width), BF16),
            pltpu.VMEM(part, BF16),
            pltpu.VMEM(part, BF16),
            pltpu.VMEM(part, BF16),
            pltpu.VMEM(part, BF16),
            pltpu.VMEM((rows, width), BF16),
            pltpu.VMEM((sp_count, 2 * top_k + -2 * top_k % 8, rows), F32),
            pltpu.VMEM((sp_count, picks, rows), BF16),
            pltpu.VMEM((sp_count, 2 * rows, picks), BF16),
            pltpu.VMEM(line, BF16),
            pltpu.VMEM(box, BF16),
            pltpu.VMEM(box, BF16),
            pltpu.VMEM(box, BF16),
            pltpu.VMEM(box, BF16),
            pltpu.VMEM(line, F32),
            pltpu.VMEM(line[1:], F32),
            pltpu.VMEM(line, BF16),
            pltpu.VMEM((2,) + line, BF16),
            dma((4,)),
            dma((chips, pieces)),
            dma((chips, pieces)),
            dma((chips, pieces)),
            dma((chips, pieces)),
            dma((sp_count,)),
            dma((sp_count,)),
            dma((2, sp_count, pieces)),
            dma((sp_count, pieces)),
            dma((sp_count, pieces, tp_count)),
            dma((sp_count, pieces, tp_count)),
            dma((sp_count, pieces, tp_count)),
            dma((sp_count, pieces, tp_count)),
            dma((sp_count, pieces)),
            dma((2, sp_count, pieces)),
        ],
        compiler_params=pltpu.CompilerParams(
            collective_id=0, has_side_effects=True, vmem_limit_bytes=VMEM_BUDGET
        ),
    )(
        queries, kv, sink_logit[None], out_weight, residual, norm_gain[None], expert_ids.T, route_weights.T,
        gate_weight, up_weight, down_weight,
    )


def on_device(queries, key_heads, value_heads, sink_logit, *rest):
    rows_dev = rest[1].shape[0]
    experts = lax.axis_size("sp") * lax.axis_size("tp")
    fits = 2 * rest[3].shape[1] * rows_dev // experts % 16 == 0 and rows_dev % WINDOW == 0
    fits = fits and lax.axis_size("sp") > 1
    if fits:
        return fused(queries, key_heads, value_heads, sink_logit, *rest)
    return tail_plain(attention(queries, key_heads, value_heads, sink_logit), *rest)


def solution(mesh):
    return jax.shard_map(
        on_device,
        mesh=mesh,
        in_specs=(
            P(("grp", "sp"), "tp"),
            P(("grp", "sp"), "tp", None),
            P(("grp", "sp"), "tp", None),
            P("tp"),
            P("tp", None),
            P(("grp", "sp", "tp"), None),
            P(),
            P(("grp", "sp", "tp"), None),
            P(("grp", "sp", "tp"), None),
            P(("sp", "tp"), None, None),
            P(("sp", "tp"), None, None),
            P(("sp", "tp"), None, None),
        ),
        out_specs=P(("grp", "sp", "tp"), None),
        check_vma=False,
    )
```

```python
import functools

import jax
import jax.numpy as jnp
from jax import lax
from jax.experimental import pallas as pl
from jax.experimental.pallas import tpu as pltpu
from jax.sharding import PartitionSpec as P

WINDOW = 128


EPS = 1e-06

F32 = jnp.float32
BF16 = jnp.bfloat16
MESH = pl.DeviceIdType.MESH
VMEM_BUDGET = 56 * 1024 * 1024


def from_behind(value, axis, steps):
    count = lax.axis_size(axis)
    initial, last = (max(0, -steps), min(count, count - steps))
    return lax.ppermute(value, axis, [(source, source + steps) for source in range(initial, last)])


def dot(a, b, dims=((1,), (0,))):
    return lax.dot_general(a, b, (dims, ((), ())), preferred_element_type=F32)


def attention(queries, key_heads, value_heads, sink_logit):
    rows_sp = queries.shape[0]
    kv_local = key_heads.shape[1]
    head_dim = key_heads.shape[2]
    heads_local = queries.shape[1] // head_dim
    group_size = heads_local // kv_local
    window = WINDOW
    count_of_blocks = rows_sp // window
    edge = jnp.stack([key_heads[rows_sp - window :], value_heads[rows_sp - window :]])
    tail_rows = from_behind(edge, "sp", 1)
    key_blocks = jnp.concatenate([tail_rows[0], key_heads], 0).reshape(
        count_of_blocks + 1, window, kv_local, head_dim
    )
    value_blocks = jnp.concatenate([tail_rows[1], value_heads], 0).reshape(
        count_of_blocks + 1, window, kv_local, head_dim
    )
    key_span = jnp.concatenate([key_blocks[:-1], key_blocks[1:]], 1)
    value_span = jnp.concatenate([value_blocks[:-1], value_blocks[1:]], 1)
    query_pos = jnp.arange(window, dtype=jnp.int32)[:, None]
    key_pos = jnp.arange(2 * window, dtype=jnp.int32)[None, :]
    distance = query_pos + window - key_pos
    band = (distance >= 0) & (distance < window)
    key_start = (
        lax.axis_index("sp") * rows_sp
        + jnp.arange(count_of_blocks, dtype=jnp.int32)[:, None] * window
        - window
        + key_pos
    )
    allowed = band[None, :, :] & (key_start >= 0)[:, None, :]
    query_blocks = queries.reshape(count_of_blocks, window, kv_local, group_size, head_dim)
    logit_scores = jnp.einsum(
        "bqhgd,bkhd->bhgqk", query_blocks, key_span, preferred_element_type=jnp.float32
    ) * head_dim ** (-0.5)
    logit_scores = jnp.where(allowed[:, None, None], logit_scores, -jnp.inf)
    sink_col = sink_logit.reshape(kv_local, group_size)[None, :, :, None, None]
    row_max = jnp.maximum(jnp.max(logit_scores, axis=-1, keepdims=True), sink_col)
    expd = jnp.exp(logit_scores - row_max)
    row_total = jnp.sum(expd, axis=-1, keepdims=True) + jnp.exp(sink_col - row_max)
    attention_probabilities = (expd / row_total).astype(jnp.bfloat16)
    attended = jnp.einsum(
        "bhgqk,bkhd->bqhgd", attention_probabilities, value_span, preferred_element_type=jnp.float32
    ).astype(jnp.bfloat16)
    return attended.reshape(rows_sp, heads_local * head_dim)


def tail_plain(
    attended, out_weight, residual, norm_gain, expert_ids, route_weights,
    gate_weight, up_weight, down_weight,
):
    rows_dev = residual.shape[0]
    width = residual.shape[1]
    projected = lax.psum_scatter(
        jnp.dot(attended, out_weight, preferred_element_type=jnp.float32),
        "tp",
        scatter_dimension=0,
        tiled=True,
    )
    stream = (residual.astype(jnp.float32) + projected).astype(jnp.bfloat16)
    wide = stream.astype(jnp.float32)
    normed = (
        wide * lax.rsqrt(jnp.mean(wide * wide, axis=-1, keepdims=True) + EPS) * norm_gain
    ).astype(jnp.bfloat16)
    sp_count = lax.axis_size("sp")
    tp_count = lax.axis_size("tp")
    experts_total = sp_count * tp_count
    top_k = expert_ids.shape[1]
    capacity = max(2, 2 * top_k * rows_dev // experts_total)
    flat_ids = expert_ids.reshape(-1)
    pairs = flat_ids.shape[0]
    onehot = (flat_ids[:, None] == jnp.arange(experts_total, dtype=jnp.int32)[None, :]).astype(
        jnp.int32
    )
    earlier = jnp.cumsum(onehot, axis=0) - onehot
    slot_rank = jnp.sum(earlier * onehot, axis=1)
    flat_slot = flat_ids * capacity + slot_rank
    owner_row = jnp.arange(pairs, dtype=jnp.int32) // top_k
    token_in_slot = jnp.zeros((experts_total * capacity,), jnp.int32).at[flat_slot].set(owner_row)
    filled = jnp.zeros((experts_total * capacity,), jnp.bool_).at[flat_slot].set(True)
    outbox = jnp.where(filled[:, None], normed[token_in_slot], jnp.zeros((), jnp.bfloat16))
    outbox = outbox.reshape(experts_total, capacity, width)
    arrived = lax.all_to_all(outbox, ("sp", "tp"), split_axis=0, concat_axis=0, tiled=True)
    rows = arrived.reshape(-1, width)
    gate = jnp.dot(rows, gate_weight[0], preferred_element_type=jnp.float32)
    upward = jnp.dot(rows, up_weight[0], preferred_element_type=jnp.float32)
    expert_hidden = (jax.nn.silu(gate) * upward).astype(jnp.bfloat16)
    expert_rows = jnp.dot(expert_hidden, down_weight[0], preferred_element_type=jnp.float32).astype(
        jnp.bfloat16
    )
    results = expert_rows.reshape(arrived.shape)
    returned = lax.all_to_all(results, ("sp", "tp"), split_axis=0, concat_axis=0, tiled=True)
    picked_rows = returned.reshape(experts_total * capacity, width)[flat_slot].reshape(
        rows_dev, top_k, width
    )
    shares = route_weights / jnp.sum(route_weights, axis=-1, keepdims=True)
    combined = jnp.sum(shares[:, :, None] * picked_rows.astype(jnp.float32), axis=1)
    return (wide + combined).astype(jnp.bfloat16)


def routing(facts, first, top_k, experts, capacity):
    facts = facts.T
    rows = facts.shape[0]
    ids, weights = facts[:, :top_k], facts[:, top_k : 2 * top_k]
    expert = (first + lax.broadcasted_iota(jnp.int32, (rows, experts), 1)).astype(F32)
    total = jnp.sum(weights, axis=1, keepdims=True)
    member = jnp.zeros((rows, experts), F32)
    share = jnp.zeros((rows, experts), F32)
    for k in range(top_k):
        hit = jnp.where(ids[:, k : k + 1] == expert, 1.0, 0.0)
        member = member + hit
        share = share + hit * (weights[:, k : k + 1] / total)
    before = (
        lax.broadcasted_iota(jnp.int32, (rows, rows), 0)
        > lax.broadcasted_iota(jnp.int32, (rows, rows), 1)
    ).astype(BF16)
    rank = dot(before, member.astype(BF16))
    rank = jnp.where(member > 0, rank, -1.0)
    slots = experts * capacity
    spread = (
        lax.broadcasted_iota(jnp.int32, (experts, slots), 1) // capacity
        == lax.broadcasted_iota(jnp.int32, (experts, slots), 0)
    ).astype(BF16)
    rank_slot = dot(rank.astype(BF16), spread)
    place = lax.broadcasted_iota(jnp.int32, (rows, slots), 1) % capacity
    taken = rank_slot == place.astype(F32)
    high = share.astype(BF16)
    low = (share - high.astype(F32)).astype(BF16)
    one = jnp.where(taken, 1.0, 0.0)
    shares = jnp.concatenate([one * dot(high, spread), one * dot(low, spread)], 0)
    return one.T.astype(BF16), shares.astype(BF16)


def attend(z, token_rows, queries, sink, seen, attended, at):
    window = WINDOW
    rows, lanes = queries.shape[0], seen.shape[1]
    heads = sink.shape[1]
    size = queries.shape[1] // heads
    groups = lanes // (2 * size)
    share = heads // groups
    pairs = share // 2
    tall = pairs * window
    query = lax.broadcasted_iota(jnp.int32, (tall, 2 * window), 0) % window
    key = lax.broadcasted_iota(jnp.int32, (tall, 2 * window), 1)
    distance = query + window - key
    band = (distance >= 0) & (distance < window)

    def block(b):
        allowed = band & ((z * rows + b * window - window) + key >= 0)
        span = seen[pl.ds(pl.multiple_of(b * window, window), 2 * window), :]
        here = pl.ds(pl.multiple_of(b * window, window), window)
        for g in range(groups):
            keys = span[:, 2 * g * size : (2 * g + 1) * size]
            values = span[:, (2 * g + 1) * size : (2 * g + 2) * size]
            none, ones = jnp.zeros_like(keys), jnp.ones_like(values)
            wide = jnp.concatenate(
                [
                    queries[here, (g * share + 2 * i) * size : (g * share + 2 * i + 2) * size]
                    for i in range(pairs)
                ],
                0,
            )
            sides = []
            for odd in range(2):
                two_keys = jnp.concatenate([none, keys] if odd else [keys, none], 1)
                two_values = jnp.concatenate([ones, values] if odd else [values, ones], 1)
                score = dot(wide, two_keys, ((1,), (1,))) * size**-0.5
                score = jnp.where(allowed, score, -1e30)
                drain = jnp.concatenate(
                    [
                        jnp.broadcast_to(
                            sink[0:1, g * share + 2 * i + odd : g * share + 2 * i + odd + 1],
                            (window, 1),
                        )
                        for i in range(pairs)
                    ],
                    0,
                )
                top = jnp.maximum(jnp.max(score, axis=1, keepdims=True), drain)
                grown = jnp.exp(score - top).astype(BF16)
                both = dot(grown, two_values)
                at = 0 if odd else size
                total = both[:, at : at + 1] + jnp.exp(drain - top)
                sides.append(both * (1.0 / total))
            lane = lax.broadcasted_iota(jnp.int32, (tall, 2 * size), 1)
            both = jnp.where(lane < size, sides[0], sides[1]).astype(BF16)
            for i in range(pairs):
                first = (g * share + 2 * i) * size
                attended[here, first : first + 2 * size] = both[i * window : (i + 1) * window]

    for b in range(token_rows // window):
        block(at * (token_rows // window) + b)


def timeline(count, pieces, favour=None):
    hop, narrow, tick = 0.6, 0.5, 0.05
    line_lead, layer_lead = 0.3, 0.6
    cost = {"pick": 0.07, "expert": 0.67, "mix": 0.08, "pass": 0.02, "norm": 0.02}
    every = range(count)
    parts = [(s, q) for s in every for q in range(pieces)]
    landed = {(d, d, q): 0.0 for d in every for q in range(pieces)}
    came, back, mixed, handed = {}, {}, {}, {}
    line, layer, busy = {}, [0.0] * count, [0.0] * count
    done = [set() for _ in every]
    steps = [[("norm", d, q) for q in range(pieces)] for d in every]
    now = 0.0

    def put(d, way, at, board, part):
        line[d, way] = max(line.get((d, way), 0.0), at) + 1
        board[(d + way,) + part] = line[d, way] + hop

    def there(board, d, part):
        return board.get((d,) + part, now + 1) <= now

    def choose(d):
        for way, name in ((-1, "send_out"), (1, "send_in")):
            if 0 <= d + way < count and line.get((d, way), 0.0) <= now + line_lead:
                ready = [
                    p
                    for p in parts
                    if (p[0] - d) * way <= 0 and there(landed, d, p) and (name, p) not in done[d]
                ]
                if ready:
                    return name, min(ready, key=lambda p: (-abs(p[0] - d), p[1]))
        ready = [
            p
            for p in parts
            if p[0] != d and there(handed, d, p) and there(mixed, d, p) and ("pass", p) not in done[d]
        ]
        if ready:
            return "pass", min(ready, key=lambda p: handed[(d,) + p])
        for p in parts:
            if there(back, d, p) and ("mix", p) not in done[d]:
                return "mix", p
        ready = [
            (s, 0)
            for s in every
            if there(came, d, (s, pieces - 1)) and ("expert", (s, 0)) not in done[d]
        ]
        if ready:
            return "expert", min(ready, key=lambda p: came[d, p[0], pieces - 1])
        ready = [p for p in parts if there(landed, d, p) and ("pick", p) not in done[d]]
        if ready and layer[d] <= now + layer_lead:
            return "pick", min(ready, key=lambda p: (favour[d][p[0]] if favour else 0, p))
        return None

    size = count * pieces
    due = [{"mix": size, "pass": size - pieces if 0 < d < count - 1 else 0} for d in every]
    while any(sum(k == name for k, _ in done[d]) < due[d][name] for d in every for name in due[d]):
        for d in every:
            while busy[d] <= now:
                step = choose(d)
                if step is None:
                    break
                name, part = step
                done[d].add(step)
                steps[d].append((name,) + part)
                busy[d] = now + cost.get(name, 0.0)
                if name == "send_in":
                    put(d, 1, now, landed, part)
                elif name == "send_out":
                    put(d, -1, now, landed, part)
                elif name == "pick":
                    layer[d] = max(layer[d], busy[d]) + narrow
                    came[(d,) + part] = layer[d] + hop
                elif name == "expert":
                    for q in range(pieces):
                        ready = now + cost[name] * (q + 3) / (pieces + 2)
                        layer[d] = max(layer[d], ready) + narrow
                        back[d, part[0], q] = layer[d] + hop
                elif name == "mix":
                    mixed[(d,) + part] = busy[d]
                if name == "pass" or (name == "mix" and part[0] != d and d in (0, count - 1)):
                    put(d, 1 if part[0] > d else -1, busy[d], handed, part)
        now += tick
    if favour is None:
        return timeline(count, pieces, [[landed[d, s, pieces - 1] for s in every] for d in every])
    return steps


def tail_kernel(
    sizes,
    queries_hbm, keys, values, sink, out_w_hbm, residual_hbm, gain, ids, weights, gate_hbm, up_hbm, down_hbm,
    out,
    queries, residual, seen, attended, halo_send, halo_recv,
    out_w, gate_w, up_w, down_w,
    pair_out, pair_in, far_out, far_in,
    stream, facts, slots, shares,
    tokens, outbox, arrived, results, returned,
    local, total_own, line_out, line_in,
    load_sem, pair_send, pair_recv, far_send, far_recv,
    facts_send, facts_recv, line_go_send, line_go_recv,
    go_send, go_recv, back_send, back_recv, line_back_send, line_back_recv,
):
    sp_count, tp_count, pieces, capacity = sizes
    chips = tp_count // 2
    z, t = lax.axis_index("sp"), lax.axis_index("tp")
    x, core = t // 2, t % 2
    other = 1 - core
    rows, width = residual_hbm.shape
    piece = width // pieces
    top_k = ids.shape[0]
    picks = tp_count * capacity

    barrier = pltpu.get_barrier_semaphore()
    for k in range(1, sp_count):
        pl.semaphore_signal(
            barrier, inc=1, device_id={"sp": (z + k) % sp_count}, device_id_type=MESH
        )
    for k in range(1, tp_count):
        pl.semaphore_signal(
            barrier, inc=1, device_id={"tp": (t + k) % tp_count}, device_id_type=MESH
        )
    loads = [
        pltpu.make_async_copy(src, dst, load_sem.at[i])
        for i, (src, dst) in enumerate(
            (
                (queries_hbm, queries), (out_w_hbm, out_w), (residual_hbm, residual),
                (gate_hbm.at[0], gate_w), (up_hbm.at[0], up_w), (down_hbm.at[0], down_w),
            )
        )
    ]
    for load in loads:
        load.start()

    groups, size, reach = keys.shape
    for g in range(groups):
        both = jnp.concatenate([keys[g], values[g]], 0)
        seen[WINDOW:, 2 * g * size : (2 * g + 2) * size] = both.T

    @pl.when(z == 0)
    def _():
        seen[:WINDOW, :] = jnp.zeros((WINDOW, seen.shape[1]), BF16)

    pad = jnp.zeros((-2 * top_k % 8, rows), F32)
    facts[z] = jnp.concatenate([ids[...].astype(F32), weights[...], pad], 0)
    pl.semaphore_wait(barrier, sp_count + tp_count - 2)
    halo_copy = pltpu.make_async_remote_copy(
        seen.at[pl.ds(reach, WINDOW)], seen.at[pl.ds(0, WINDOW)], halo_send, halo_recv,
        device_id={"sp": jnp.minimum(z + 1, sp_count - 1)}, device_id_type=MESH,
    )

    @pl.when(z < sp_count - 1)
    def _():
        halo_copy.start()

    def facts_copy(k):
        return pltpu.make_async_remote_copy(
            facts.at[z], facts.at[z], facts_send, facts_recv.at[z],
            device_id={"sp": (z + k) % sp_count}, device_id_type=MESH,
        )

    def facts_wait(s):
        pltpu.make_async_remote_copy(
            facts.at[s], facts.at[s], facts_send, facts_recv.at[s],
            device_id={"sp": s}, device_id_type=MESH,
        ).wait_recv()

    for k in range(1, sp_count):
        facts_copy(k).start()

    def route(s):
        slots[s], shares[s] = routing(facts[s], z * tp_count, top_k, tp_count, capacity)

    loads[0].wait()

    def attend_block(at):
        @pl.when((z > 0) & (at == 0))
        def _():
            halo_copy.wait_recv()

        attend(z, rows, queries, sink, seen, attended, at)

    def partial(chip, which, q):
        block = attended[pl.ds(pl.multiple_of((chip * 2 + which) * rows, rows), rows), :]
        return dot(block, out_w[:, q * piece : (q + 1) * piece])

    def pair_copy(k, q):
        return pltpu.make_async_remote_copy(
            pair_out.at[k, q], pair_in.at[k, q], pair_send, pair_recv.at[k, q],
            device_id={"tp": x * 2 + other}, device_id_type=MESH,
        )

    def far_copy(k, q):
        return pltpu.make_async_remote_copy(
            far_out.at[k, q], far_in.at[k, q], far_send, far_recv.at[k, q],
            device_id={"tp": ((x + k) % chips) * 2 + core}, device_id_type=MESH,
        )

    order = list(range(1, chips)) + [0]
    for k in order:
        chip = (x + k) % chips
        attend_block(chip * 2 + other)
        if k == order[0]:
            loads[1].wait()
        for q in range(pieces):
            pair_out[k, q] = partial(chip, other, q).astype(BF16)
            pair_copy(k, q).start()
        attend_block(chip * 2 + core)
        for q in range(pieces if k else 0):
            mine = partial(chip, core, q)
            pair_copy(k, q).wait_recv()
            far_out[k, q] = (mine + pair_in[k, q].astype(F32)).astype(BF16)
            far_copy(k, q).start()

    def route_other(k, carry):
        s = (z + k) % sp_count
        facts_wait(s)
        route(s)
        return carry

    route(z)
    loads[2].wait()
    lax.fori_loop(1, sp_count, route_other, 0)
    square = jnp.zeros((rows, 1), F32)
    for q in range(pieces):
        cols = slice(q * piece, (q + 1) * piece)
        total = partial(x, core, q)
        pair_copy(0, q).wait_recv()
        total = total + pair_in[0, q].astype(F32)
        for k in range(1, chips):
            far_copy(k, q).wait_recv()
            total = total + far_in[k, q].astype(F32)
        value = (residual[:, cols].astype(F32) + total).astype(BF16)
        stream[:, cols] = value
        value = value.astype(F32)
        square = square + jnp.sum(value * value, axis=1, keepdims=True)
    scale = lax.rsqrt(square / width + EPS)

    def line_go(to, s, q):
        return pltpu.make_async_remote_copy(
            tokens.at[s, q], tokens.at[s, q], line_go_send, line_go_recv.at[s, q],
            device_id={"sp": to}, device_id_type=MESH,
        )

    def line_back(to, s, q, way):
        return pltpu.make_async_remote_copy(
            line_out.at[s, q], line_in.at[way, s, q], line_back_send,
            line_back_recv.at[way, s, q], device_id={"sp": to}, device_id_type=MESH,
        )

    def go_copy(s, q, to, at):
        return pltpu.make_async_remote_copy(
            outbox.at[s, q, to], arrived.at[s, q, at], go_send, go_recv.at[s, q],
            device_id={"tp": to}, device_id_type=MESH,
        )

    def back_copy(s, q, to, at):
        return pltpu.make_async_remote_copy(
            results.at[s, q, to], returned.at[s, q, at], back_send, back_recv.at[s, q],
            device_id={"tp": to}, device_id_type=MESH,
        )

    def box_wait(box, send, recv, s, q):
        part = pl.ds(0, tp_count - 1)
        pltpu.make_async_remote_copy(
            box.at[s, q, part], box.at[s, q, part], send, recv.at[s, q],
            device_id={"tp": (t + 1) % tp_count}, device_id_type=MESH,
        ).wait_recv()

    def sent(ref, send, peer):
        pltpu.make_async_remote_copy(
            ref, ref, send, halo_recv, device_id=peer, device_id_type=MESH
        ).wait_send()

    peers = [(t + k) % tp_count for k in range(1, tp_count)]
    flip = (z * 2 >= sp_count).astype(jnp.int32)
    place = z + flip * (sp_count - 1 - 2 * z)

    def real(s):
        return s + flip * (sp_count - 1 - 2 * s)

    def program(m):
        inner, outer = flip, 1 - flip

        def norm(s, q):
            cols = slice(q * piece, (q + 1) * piece)
            tokens[z, q] = (stream[:, cols].astype(F32) * scale * gain[:, cols]).astype(BF16)

        def land(s, q):
            line_go(real(s), real(s), q).wait_recv()

        def send_in(s, q):
            line_go(real(m + 1), real(s), q).start()

        def send_out(s, q):
            line_go(real(m - 1), real(s), q).start()

        def pick(s, q):
            r = real(s)
            chosen = dot(slots[r], tokens[r, q]).astype(BF16)
            outbox[r, q] = chosen.reshape(tp_count, capacity, piece)
            for to in peers:
                go_copy(r, q, to, t).start()
            arrived[r, q, t] = outbox[r, q, t]

        def expert(s, _):
            r = real(s)
            gated = raised = None
            for q in range(pieces):
                box_wait(arrived, go_send, go_recv, r, q)
                block = arrived[r, q].reshape(picks, piece)
                part = slice(q * piece, (q + 1) * piece)
                a, b = dot(block, gate_w[part, :]), dot(block, up_w[part, :])
                gated, raised = (a, b) if q == 0 else (gated + a, raised + b)
            hidden = (gated / (1.0 + jnp.exp(-gated)) * raised).astype(BF16)
            for q in range(pieces):
                done = dot(hidden, down_w[:, q * piece : (q + 1) * piece]).astype(BF16)
                results[r, q] = done.reshape(tp_count, capacity, piece)
                for to in peers:
                    back_copy(r, q, to, t).start()
                returned[r, q, t] = results[r, q, t]

        def mix(s, q):
            r = real(s)
            box_wait(returned, back_send, back_recv, r, q)
            both = dot(shares[r], returned[r, q].reshape(picks, piece))
            mixed = both[:rows] + both[rows:]
            if s == m:
                total_own[q] = stream[:, q * piece : (q + 1) * piece].astype(F32) + mixed
            elif m == 0:
                line_out[r, q] = mixed.astype(BF16)
                line_back(real(1), r, q, inner).start()
            else:
                local[r, q] = mixed

        def hand_on(s, q):
            r = real(s)
            way, to = (inner, m + 1) if s > m else (outer, m - 1)
            line_back(real(to), r, q, way).wait_recv()
            line_out[r, q] = (local[r, q] + line_in[way, r, q].astype(F32)).astype(BF16)
            line_back(real(to), r, q, way).start()

        act = {
            "norm": norm, "send_in": send_in, "send_out": send_out,
            "pick": pick, "expert": expert, "mix": mix, "pass": hand_on,
        }
        waited = set()
        for name, s, q in steps[m]:
            if name == "expert" and "loads" not in waited:
                waited.add("loads")
                for load in loads[3:]:
                    load.wait()
            if name in ("pick", "send_in", "send_out") and s != m and (s, q) not in waited:
                waited.add((s, q))
                land(s, q)
            act[name](s, q)
        for q in range(pieces):
            total = total_own[q]
            for way in [inner, outer] if m > 0 else [outer]:
                line_back(real(m + 1), z, q, way).wait_recv()
                total = total + line_in[way, z, q].astype(F32)
            out[:, q * piece : (q + 1) * piece] = total.astype(BF16)
        peer = {"sp": real(m + 1)}
        for _ in range(sp_count + 1 if m > 0 else 1):
            sent(tokens.at[0], line_go_send, peer)
        sent(line_out.at[pl.ds(0, sp_count - 1)], line_back_send, peer)

    steps = timeline(sp_count, pieces)
    for m in range((sp_count + 1) // 2):
        pl.when(place == m)(functools.partial(program, m))

    @pl.when(z < sp_count - 1)
    def _():
        halo_copy.wait_send()

    peer = {"tp": x * 2 + other}
    sent(facts.at[pl.ds(0, sp_count - 1)], facts_send, {"sp": (z + 1) % sp_count})
    sent(pair_out, pair_send, peer)
    sent(far_out.at[pl.ds(1, chips - 1)], far_send, peer)
    sent(outbox.at[:, :, pl.ds(0, tp_count - 1)], go_send, peer)
    sent(results.at[:, :, pl.ds(0, tp_count - 1)], back_send, peer)


def fused(
    queries, key_heads, value_heads, sink_logit, out_weight, residual, norm_gain, expert_ids, route_weights,
    gate_weight, up_weight, down_weight,
):
    rows, width = residual.shape
    sp_count, tp_count = lax.axis_size("sp"), lax.axis_size("tp")
    experts = sp_count * tp_count
    top_k = expert_ids.shape[1]
    capacity = max(2, 2 * top_k * rows // experts)
    hidden = gate_weight.shape[2]
    depth = out_weight.shape[0]
    pieces = 4
    chips = tp_count // 2
    piece = width // pieces
    part = (chips, pieces, rows, piece)
    line = (sp_count, pieces, rows, piece)
    box = (sp_count, pieces, tp_count, capacity, piece)
    picks = tp_count * capacity
    reach, groups, size = key_heads.shape
    keys, values = key_heads.transpose(1, 2, 0), value_heads.transpose(1, 2, 0)
    vmem = pl.BlockSpec(memory_space=pltpu.VMEM)
    hbm = pl.BlockSpec(memory_space=pl.ANY)
    dma = pltpu.SemaphoreType.DMA
    return pl.pallas_call(
        functools.partial(tail_kernel, (sp_count, tp_count, pieces, capacity)),
        out_shape=jax.ShapeDtypeStruct((rows, width), BF16),
        in_specs=[hbm, vmem, vmem, vmem, hbm, hbm, vmem, vmem, vmem, hbm, hbm, hbm],
        out_specs=vmem,
        scratch_shapes=[
            pltpu.VMEM(queries.shape, BF16),
            pltpu.VMEM(residual.shape, BF16),
            pltpu.VMEM((WINDOW + reach, groups * 2 * size), BF16),
            pltpu.VMEM(queries.shape, BF16),
            dma,
            dma,
            pltpu.VMEM((depth, width), BF16),
            pltpu.VMEM((width, hidden), BF16),
            pltpu.VMEM((width, hidden), BF16),
            pltpu.VMEM((hidden, width), BF16),
            pltpu.VMEM(part, BF16),
            pltpu.VMEM(part, BF16),
            pltpu.VMEM(part, BF16),
            pltpu.VMEM(part, BF16),
            pltpu.VMEM((rows, width), BF16),
            pltpu.VMEM((sp_count, 2 * top_k + -2 * top_k % 8, rows), F32),
            pltpu.VMEM((sp_count, picks, rows), BF16),
            pltpu.VMEM((sp_count, 2 * rows, picks), BF16),
            pltpu.VMEM(line, BF16),
            pltpu.VMEM(box, BF16),
            pltpu.VMEM(box, BF16),
            pltpu.VMEM(box, BF16),
            pltpu.VMEM(box, BF16),
            pltpu.VMEM(line, F32),
            pltpu.VMEM(line[1:], F32),
            pltpu.VMEM(line, BF16),
            pltpu.VMEM((2,) + line, BF16),
            dma((6,)),
            dma,
            dma((chips, pieces)),
            dma,
            dma((chips, pieces)),
            dma,
            dma((sp_count,)),
            dma,
            dma((sp_count, pieces)),
            dma,
            dma((sp_count, pieces)),
            dma,
            dma((sp_count, pieces)),
            dma,
            dma((2, sp_count, pieces)),
        ],
        compiler_params=pltpu.CompilerParams(
            collective_id=0, has_side_effects=True, vmem_limit_bytes=VMEM_BUDGET
        ),
    )(
        queries, keys, values, sink_logit[None], out_weight, residual, norm_gain[None], expert_ids.T, route_weights.T,
        gate_weight, up_weight, down_weight,
    )


def on_device(queries, key_heads, value_heads, sink_logit, *rest):
    rows_dev = rest[1].shape[0]
    experts = lax.axis_size("sp") * lax.axis_size("tp")
    fits = 2 * rest[3].shape[1] * rows_dev // experts % 16 == 0 and rows_dev % WINDOW == 0
    fits = fits and lax.axis_size("sp") > 1 and lax.axis_size("tp") > 2
    if fits:
        return fused(queries, key_heads, value_heads, sink_logit, *rest)
    return tail_plain(attention(queries, key_heads, value_heads, sink_logit), *rest)


def solution(mesh):
    return jax.shard_map(
        on_device,
        mesh=mesh,
        in_specs=(
            P(("grp", "sp"), "tp"),
            P(("grp", "sp"), "tp", None),
            P(("grp", "sp"), "tp", None),
            P("tp"),
            P("tp", None),
            P(("grp", "sp", "tp"), None),
            P(),
            P(("grp", "sp", "tp"), None),
            P(("grp", "sp", "tp"), None),
            P(("sp", "tp"), None, None),
            P(("sp", "tp"), None, None),
            P(("sp", "tp"), None, None),
        ),
        out_specs=P(("grp", "sp", "tp"), None),
        check_vma=False,
    )
```

```python
import functools

import jax
import jax.numpy as jnp
from jax import lax
from jax.experimental import pallas as pl
from jax.experimental.pallas import tpu as pltpu
from jax.sharding import PartitionSpec as P

WINDOW = 128


EPS = 1e-06

F32 = jnp.float32
BF16 = jnp.bfloat16
MESH = pl.DeviceIdType.MESH
VMEM_BUDGET = 56 * 1024 * 1024


def from_behind(value, axis, steps):
    count = lax.axis_size(axis)
    initial, last = (max(0, -steps), min(count, count - steps))
    return lax.ppermute(value, axis, [(source, source + steps) for source in range(initial, last)])


def dot(a, b, dims=((1,), (0,))):
    return lax.dot_general(a, b, (dims, ((), ())), preferred_element_type=F32)


def attention(queries, key_heads, value_heads, sink_logit):
    rows_sp = queries.shape[0]
    kv_local = key_heads.shape[1]
    head_dim = key_heads.shape[2]
    heads_local = queries.shape[1] // head_dim
    group_size = heads_local // kv_local
    window = WINDOW
    count_of_blocks = rows_sp // window
    edge = jnp.stack([key_heads[rows_sp - window :], value_heads[rows_sp - window :]])
    tail_rows = from_behind(edge, "sp", 1)
    key_blocks = jnp.concatenate([tail_rows[0], key_heads], 0).reshape(
        count_of_blocks + 1, window, kv_local, head_dim
    )
    value_blocks = jnp.concatenate([tail_rows[1], value_heads], 0).reshape(
        count_of_blocks + 1, window, kv_local, head_dim
    )
    key_span = jnp.concatenate([key_blocks[:-1], key_blocks[1:]], 1)
    value_span = jnp.concatenate([value_blocks[:-1], value_blocks[1:]], 1)
    query_pos = jnp.arange(window, dtype=jnp.int32)[:, None]
    key_pos = jnp.arange(2 * window, dtype=jnp.int32)[None, :]
    distance = query_pos + window - key_pos
    band = (distance >= 0) & (distance < window)
    key_start = (
        lax.axis_index("sp") * rows_sp
        + jnp.arange(count_of_blocks, dtype=jnp.int32)[:, None] * window
        - window
        + key_pos
    )
    allowed = band[None, :, :] & (key_start >= 0)[:, None, :]
    query_blocks = queries.reshape(count_of_blocks, window, kv_local, group_size, head_dim)
    logit_scores = jnp.einsum(
        "bqhgd,bkhd->bhgqk", query_blocks, key_span, preferred_element_type=jnp.float32
    ) * head_dim ** (-0.5)
    logit_scores = jnp.where(allowed[:, None, None], logit_scores, -jnp.inf)
    sink_col = sink_logit.reshape(kv_local, group_size)[None, :, :, None, None]
    row_max = jnp.maximum(jnp.max(logit_scores, axis=-1, keepdims=True), sink_col)
    expd = jnp.exp(logit_scores - row_max)
    row_total = jnp.sum(expd, axis=-1, keepdims=True) + jnp.exp(sink_col - row_max)
    attention_probabilities = (expd / row_total).astype(jnp.bfloat16)
    attended = jnp.einsum(
        "bhgqk,bkhd->bqhgd", attention_probabilities, value_span, preferred_element_type=jnp.float32
    ).astype(jnp.bfloat16)
    return attended.reshape(rows_sp, heads_local * head_dim)


def tail_plain(
    attended, out_weight, residual, norm_gain, expert_ids, route_weights,
    gate_weight, up_weight, down_weight,
):
    rows_dev = residual.shape[0]
    width = residual.shape[1]
    projected = lax.psum_scatter(
        jnp.dot(attended, out_weight, preferred_element_type=jnp.float32),
        "tp",
        scatter_dimension=0,
        tiled=True,
    )
    stream = (residual.astype(jnp.float32) + projected).astype(jnp.bfloat16)
    wide = stream.astype(jnp.float32)
    normed = (
        wide * lax.rsqrt(jnp.mean(wide * wide, axis=-1, keepdims=True) + EPS) * norm_gain
    ).astype(jnp.bfloat16)
    sp_count = lax.axis_size("sp")
    tp_count = lax.axis_size("tp")
    experts_total = sp_count * tp_count
    top_k = expert_ids.shape[1]
    capacity = max(2, 2 * top_k * rows_dev // experts_total)
    flat_ids = expert_ids.reshape(-1)
    pairs = flat_ids.shape[0]
    onehot = (flat_ids[:, None] == jnp.arange(experts_total, dtype=jnp.int32)[None, :]).astype(
        jnp.int32
    )
    earlier = jnp.cumsum(onehot, axis=0) - onehot
    slot_rank = jnp.sum(earlier * onehot, axis=1)
    flat_slot = flat_ids * capacity + slot_rank
    owner_row = jnp.arange(pairs, dtype=jnp.int32) // top_k
    token_in_slot = jnp.zeros((experts_total * capacity,), jnp.int32).at[flat_slot].set(owner_row)
    filled = jnp.zeros((experts_total * capacity,), jnp.bool_).at[flat_slot].set(True)
    outbox = jnp.where(filled[:, None], normed[token_in_slot], jnp.zeros((), jnp.bfloat16))
    outbox = outbox.reshape(experts_total, capacity, width)
    arrived = lax.all_to_all(outbox, ("sp", "tp"), split_axis=0, concat_axis=0, tiled=True)
    rows = arrived.reshape(-1, width)
    gate = jnp.dot(rows, gate_weight[0], preferred_element_type=jnp.float32)
    upward = jnp.dot(rows, up_weight[0], preferred_element_type=jnp.float32)
    expert_hidden = (jax.nn.silu(gate) * upward).astype(jnp.bfloat16)
    expert_rows = jnp.dot(expert_hidden, down_weight[0], preferred_element_type=jnp.float32).astype(
        jnp.bfloat16
    )
    results = expert_rows.reshape(arrived.shape)
    returned = lax.all_to_all(results, ("sp", "tp"), split_axis=0, concat_axis=0, tiled=True)
    picked_rows = returned.reshape(experts_total * capacity, width)[flat_slot].reshape(
        rows_dev, top_k, width
    )
    shares = route_weights / jnp.sum(route_weights, axis=-1, keepdims=True)
    combined = jnp.sum(shares[:, :, None] * picked_rows.astype(jnp.float32), axis=1)
    return (wide + combined).astype(jnp.bfloat16)


def routing(facts, first, top_k, experts, capacity):
    facts = facts.T
    rows = facts.shape[0]
    ids, weights = facts[:, :top_k], facts[:, top_k : 2 * top_k]
    expert = (first + lax.broadcasted_iota(jnp.int32, (rows, experts), 1)).astype(F32)
    total = jnp.sum(weights, axis=1, keepdims=True)
    member = jnp.zeros((rows, experts), F32)
    share = jnp.zeros((rows, experts), F32)
    for k in range(top_k):
        hit = jnp.where(ids[:, k : k + 1] == expert, 1.0, 0.0)
        member = member + hit
        share = share + hit * (weights[:, k : k + 1] / total)
    before = (
        lax.broadcasted_iota(jnp.int32, (rows, rows), 0)
        > lax.broadcasted_iota(jnp.int32, (rows, rows), 1)
    ).astype(BF16)
    rank = dot(before, member.astype(BF16))
    rank = jnp.where(member > 0, rank, -1.0)
    slots = experts * capacity
    spread = (
        lax.broadcasted_iota(jnp.int32, (experts, slots), 1) // capacity
        == lax.broadcasted_iota(jnp.int32, (experts, slots), 0)
    ).astype(BF16)
    rank_slot = dot(rank.astype(BF16), spread)
    place = lax.broadcasted_iota(jnp.int32, (rows, slots), 1) % capacity
    taken = rank_slot == place.astype(F32)
    high = share.astype(BF16)
    low = (share - high.astype(F32)).astype(BF16)
    one = jnp.where(taken, 1.0, 0.0)
    shares = jnp.concatenate([one * dot(high, spread), one * dot(low, spread)], 0)
    return one.T.astype(BF16), shares.astype(BF16)


def attend(z, queries, sink, seen, attended, first, count):
    window = WINDOW
    rows, lanes = queries.shape[0], seen.shape[1]
    heads = sink.shape[1]
    size = queries.shape[1] // heads
    groups = lanes // (2 * size)
    share = heads // groups
    pairs = share // 2
    tall, reach = pairs * count, window + count
    query = lax.broadcasted_iota(jnp.int32, (tall, reach), 0) % count
    key = lax.broadcasted_iota(jnp.int32, (tall, reach), 1)
    distance = query + window - key
    allowed = (distance >= 0) & (distance < window) & ((z * rows + first - window) + key >= 0)
    span = seen[pl.ds(pl.multiple_of(first, count), reach), :]
    here = pl.ds(pl.multiple_of(first, count), count)
    for g in range(groups):
        keys = span[:, 2 * g * size : (2 * g + 1) * size]
        values = span[:, (2 * g + 1) * size : (2 * g + 2) * size]
        none, ones = jnp.zeros_like(keys), jnp.ones_like(values)
        wide = jnp.concatenate(
            [
                queries[here, (g * share + 2 * i) * size : (g * share + 2 * i + 2) * size]
                for i in range(pairs)
            ],
            0,
        )
        sides = []
        for odd in range(2):
            two_keys = jnp.concatenate([none, keys] if odd else [keys, none], 1)
            two_values = jnp.concatenate([ones, values] if odd else [values, ones], 1)
            score = dot(wide, two_keys, ((1,), (1,))) * size**-0.5
            score = jnp.where(allowed, score, -1e30)
            drain = jnp.concatenate(
                [
                    jnp.broadcast_to(
                        sink[0:1, g * share + 2 * i + odd : g * share + 2 * i + odd + 1],
                        (count, 1),
                    )
                    for i in range(pairs)
                ],
                0,
            )
            top = jnp.maximum(jnp.max(score, axis=1, keepdims=True), drain)
            grown = jnp.exp(score - top).astype(BF16)
            both = dot(grown, two_values)
            at = 0 if odd else size
            total = both[:, at : at + 1] + jnp.exp(drain - top)
            sides.append(both * (1.0 / total))
        lane = lax.broadcasted_iota(jnp.int32, (tall, 2 * size), 1)
        both = jnp.where(lane < size, sides[0], sides[1]).astype(BF16)
        for i in range(pairs):
            at = (g * share + 2 * i) * size
            attended[here, at : at + 2 * size] = both[i * count : (i + 1) * count]


def timeline(count, pieces, halves, favour=None):
    hop, narrow, tick = 0.7, 0.5, 0.05
    line_lead, layer_lead, begun, spare = 0.3, 0.3, 1.9, 0.3
    cost = {"close": 0.2, "pick": 0.07, "expert": 0.67, "mix": 0.08, "pass": 0.02}
    every = range(count)
    bits = [(s, p) for s in every for p in range(halves * pieces)]
    parts = [(s, q) for s in every for q in range(pieces)]
    landed, came, worked, back, mixed, handed = {}, {}, {}, {}, {}, {}
    line, layer, busy = {}, [1.1] * count, [begun] * count
    done = [set() for _ in every]
    steps = [[] for _ in every]
    now = 0.0

    def put(d, way, at, board, part, size):
        line[d, way] = max(line.get((d, way), 0.0), at) + size
        key = (d + way,) + part
        board[key] = max(board.get(key, 0.0), line[d, way] + hop)

    def there(board, d, part):
        return board.get((d,) + part, now + 1) <= now

    def whole(d, p):
        return all(there(landed, d, (p[0], h * pieces + p[1])) for h in range(halves))

    def choose(d):
        for way, name in ((-1, "send_out"), (1, "send_in")):
            if 0 <= d + way < count and line.get((d, way), 0.0) <= now + line_lead:
                ready = [
                    p
                    for p in bits
                    if (p[0] - d) * way <= 0 and there(landed, d, p) and (name, p) not in done[d]
                ]
                if ready:
                    end = d + way in (0, count - 1)
                    return name, min(ready, key=lambda p: (end and p[0] == d, abs(p[0] - d), p[1]))
        if ("close", (d, 0)) not in done[d]:
            return "close", (d, 0)
        ready = [
            p
            for p in parts
            if p[0] != d and there(handed, d, p) and there(mixed, d, p) and ("pass", p) not in done[d]
        ]
        if ready:
            return "pass", min(ready, key=lambda p: handed[(d,) + p])
        for p in parts:
            if there(back, d, p) and ("mix", p) not in done[d]:
                return "mix", p
        ready = [
            (s, 0)
            for s in every
            if there(came, d, (s, pieces - 1)) and ("expert", (s, 0)) not in done[d]
        ]
        if ready:
            return "expert", min(ready, key=lambda p: came[d, p[0], pieces - 1])
        ready = [p for p in parts if whole(d, p) and ("pick", p) not in done[d]]
        if ready and layer[d] <= now + layer_lead:
            return "pick", min(ready, key=lambda p: (favour[d][p[0]] if favour else 0, p))
        ready = [p for p in parts if p[0] == d and there(worked, d, p) and ("back", p) not in done[d]]
        if ready and layer[d] <= now:
            return "back", ready[0]
        return None

    for d in every:
        for p in range(pieces):
            landed[d, d, p] = 0.0
            for way, name in ((-1, "send_out"), (1, "send_in")):
                if 0 <= d + way < count:
                    put(d, way, 0.0, landed, (d, p), 1 / halves)
                    done[d].add((name, (d, p)))
    size = count * pieces
    due = [{"mix": size, "pass": size - pieces if 0 < d < count - 1 else 0} for d in every]
    while any(sum(k == name for k, _ in done[d]) < due[d][name] for d in every for name in due[d]):
        for d in every:
            while busy[d] <= now:
                step = choose(d)
                if step is None:
                    break
                name, part = step
                done[d].add(step)
                steps[d].append((name,) + part)
                busy[d] = now + cost.get(name, 0.0)
                if name == "send_in":
                    put(d, 1, now, landed, part, 1 / halves)
                elif name == "send_out":
                    put(d, -1, now, landed, part, 1 / halves)
                elif name == "close":
                    for p in range(pieces, halves * pieces):
                        landed[d, d, p] = busy[d]
                elif name == "pick":
                    layer[d] = max(layer[d], busy[d]) + narrow
                    came[(d,) + part] = layer[d] + hop + (spare if 0 < d < count - 1 else 0)
                elif name == "expert":
                    for q in range(pieces):
                        if part[0] == d:
                            worked[d, d, q] = busy[d]
                            continue
                        ready = now + cost[name] * (q + 3) / (pieces + 2)
                        layer[d] = max(layer[d], ready) + narrow
                        back[d, part[0], q] = layer[d] + hop
                elif name == "back":
                    layer[d] = max(layer[d], now) + narrow
                    back[(d,) + part] = layer[d] + hop
                elif name == "mix":
                    mixed[(d,) + part] = busy[d]
                if name == "pass" or (name == "mix" and part[0] != d and d in (0, count - 1)):
                    put(d, 1 if part[0] > d else -1, busy[d], handed, part, 1)
        now += tick
    if favour is None:
        ends = [[landed[d, s, halves * pieces - 1] for s in every] for d in every]
        return timeline(count, pieces, halves, ends)
    return steps


def tail_kernel(
    sizes,
    queries_hbm, keys, values, sink, out_w_hbm, residual_hbm, gain, ids, weights, gate_hbm, up_hbm, down_hbm,
    out,
    queries, residual, seen, attended, halo_send, halo_recv,
    out_w, gate_w, up_w, down_w,
    pair_out, pair_in, far_out, far_in, mine,
    stream, facts, slots, shares,
    tokens, outbox, arrived, results, returned,
    local, total_own, line_out, line_in, result,
    load_sem, out_sem, pair_send, pair_recv, far_send, far_recv,
    facts_send, facts_recv, line_go_send, line_go_recv,
    go_send, go_recv, back_send, back_recv, line_back_send, line_back_recv,
):
    sp_count, tp_count, pieces, halves, capacity = sizes
    chips = tp_count // 2
    z, t = lax.axis_index("sp"), lax.axis_index("tp")
    x, core = t // 2, t % 2
    other = 1 - core
    rows, width = residual_hbm.shape
    piece, half = width // pieces, rows // halves
    top_k = ids.shape[0]
    picks = tp_count * capacity

    barrier = pltpu.get_barrier_semaphore()
    for k in range(1, sp_count):
        pl.semaphore_signal(
            barrier, inc=1, device_id={"sp": (z + k) % sp_count}, device_id_type=MESH
        )
    for k in range(1, tp_count):
        pl.semaphore_signal(
            barrier, inc=1, device_id={"tp": (t + k) % tp_count}, device_id_type=MESH
        )
    loads = [
        pltpu.make_async_copy(src, dst, load_sem.at[i])
        for i, (src, dst) in enumerate(
            (
                (queries_hbm, queries), (out_w_hbm, out_w), (residual_hbm, residual),
                (gate_hbm.at[0], gate_w), (up_hbm.at[0], up_w), (down_hbm.at[0], down_w),
            )
        )
    ]
    for load in loads:
        load.start()

    groups, size, reach = keys.shape
    for g in range(groups):
        both = jnp.concatenate([keys[g], values[g]], 0)
        seen[WINDOW:, 2 * g * size : (2 * g + 2) * size] = both.T

    @pl.when(z == 0)
    def _():
        seen[:WINDOW, :] = jnp.zeros((WINDOW, seen.shape[1]), BF16)

    pad = jnp.zeros((-2 * top_k % 8, rows), F32)
    facts[z] = jnp.concatenate([ids[...].astype(F32), weights[...], pad], 0)
    def facts_copy(k):
        return pltpu.make_async_remote_copy(
            facts.at[z], facts.at[z], facts_send, facts_recv.at[z],
            device_id={"sp": (z + k) % sp_count}, device_id_type=MESH,
        )

    def facts_wait(s):
        pltpu.make_async_remote_copy(
            facts.at[s], facts.at[s], facts_send, facts_recv.at[s],
            device_id={"sp": s}, device_id_type=MESH,
        ).wait_recv()

    def route(s):
        slots[s], shares[s] = routing(facts[s], z * tp_count, top_k, tp_count, capacity)

    halo_copy = pltpu.make_async_remote_copy(
        seen.at[pl.ds(reach, WINDOW)], seen.at[pl.ds(0, WINDOW)], halo_send, halo_recv,
        device_id={"sp": jnp.minimum(z + 1, sp_count - 1)}, device_id_type=MESH,
    )

    def attend_half(at, h):
        attend(z, queries, sink, seen, attended, at * rows + h * half, half)

    def pair_copy(h, k, q):
        return pltpu.make_async_remote_copy(
            pair_out.at[h, k, q], pair_in.at[h, k, q], pair_send, pair_recv.at[h, k, q],
            device_id={"tp": x * 2 + other}, device_id_type=MESH,
        )

    def far_copy(h, q):
        return pltpu.make_async_remote_copy(
            far_out.at[h, q], far_in.at[h, q], far_send, far_recv.at[h, q],
            device_id={"tp": (1 - x) * 2 + core}, device_id_type=MESH,
        )

    def give(h, k):
        block = jnp.concatenate(
            [
                attended[pl.ds(pl.multiple_of(at * rows + h * half, half), half), :]
                for at in ((x + k) % chips * 2 + other, (x + k) % chips * 2 + core)
            ],
            0,
        )
        for q in range(pieces):
            both = dot(block, out_w[:, q * piece : (q + 1) * piece])
            pair_out[h, k, q] = both[:half].astype(BF16)
            pair_copy(h, k, q).start()
            mine[h, k, q] = both[half:]

        @pl.when(k > 0)
        def _():
            for q in range(pieces):
                pair_copy(h, k, q).wait_recv()
                far_out[h, q] = (mine[h, k, q] + pair_in[h, k, q].astype(F32)).astype(BF16)
                far_copy(h, q).start()

    def turn(h, k):
        chip = (x + k) % chips
        attend_half(chip * 2 + 1, h)

        @pl.when((z > 0) & (chip == 0) & (h == 0))
        def _():
            halo_copy.wait_recv()

        attend_half(chip * 2, h)
        give(h, k)

    def close(h):
        here = slice(h * half, (h + 1) * half)
        square = jnp.zeros((half, 1), F32)
        for q in range(pieces):
            cols = slice(q * piece, (q + 1) * piece)
            total = mine[h, 0, q]
            pair_copy(h, 0, q).wait_recv()
            total = total + pair_in[h, 0, q].astype(F32)
            far_copy(h, q).wait_recv()
            total = total + far_in[h, q].astype(F32)
            value = (residual[here, cols].astype(F32) + total).astype(BF16)
            stream[here, cols] = value
            value = value.astype(F32)
            square = square + jnp.sum(value * value, axis=1, keepdims=True)
        scale = lax.rsqrt(square / width + EPS)
        for q in range(pieces):
            cols = slice(q * piece, (q + 1) * piece)
            tokens[z, q, here, :] = (stream[here, cols].astype(F32) * scale * gain[:, cols]).astype(BF16)

    def route_other(k, carry):
        s = (z + k) % sp_count
        facts_wait(s)
        route(s)
        return carry

    def line_go(to, s, p):
        bit = tokens.at[s, p % pieces, pl.ds(p // pieces * half, half)]
        return pltpu.make_async_remote_copy(
            bit, bit, line_go_send, line_go_recv.at[s, p],
            device_id={"sp": to}, device_id_type=MESH,
        )

    def line_back(to, s, q, way):
        return pltpu.make_async_remote_copy(
            line_out.at[s, q], line_in.at[way, s, q], line_back_send,
            line_back_recv.at[way, s, q], device_id={"sp": to}, device_id_type=MESH,
        )

    def go_copy(s, q, to, at):
        return pltpu.make_async_remote_copy(
            outbox.at[s, q, to], arrived.at[s, q, at], go_send, go_recv.at[s, q],
            device_id={"tp": to}, device_id_type=MESH,
        )

    def back_copy(s, q, to, at):
        return pltpu.make_async_remote_copy(
            results.at[s, q, to], returned.at[s, q, at], back_send, back_recv.at[s, q],
            device_id={"tp": to}, device_id_type=MESH,
        )

    def box_wait(box, send, recv, s, q):
        part = pl.ds(0, tp_count - 1)
        pltpu.make_async_remote_copy(
            box.at[s, q, part], box.at[s, q, part], send, recv.at[s, q],
            device_id={"tp": (t + 1) % tp_count}, device_id_type=MESH,
        ).wait_recv()

    def sent(ref, send, peer):
        pltpu.make_async_remote_copy(
            ref, ref, send, halo_recv, device_id=peer, device_id_type=MESH
        ).wait_send()

    peers = [(t + k) % tp_count for k in range(1, tp_count)]
    flip = (z * 2 >= sp_count).astype(jnp.int32)
    place = z + flip * (sp_count - 1 - 2 * z)

    def real(s):
        return s + flip * (sp_count - 1 - 2 * s)

    loads[0].wait()
    attend_half((chips - 1) * 2 + 1, 0)
    attend_half((chips - 1) * 2, 0)
    pl.semaphore_wait(barrier, sp_count + tp_count - 2)

    @pl.when(z < sp_count - 1)
    def _():
        halo_copy.start()

    for k in range(1, sp_count):
        facts_copy(k).start()
    loads[1].wait()
    give(0, 1 - x)

    def middle(i, carry):
        turn((1 - x) * (1 - i) + x * i, (1 - i) + x * i)
        return carry

    lax.fori_loop(0, 2, middle, 0)
    loads[2].wait()
    close(0)
    for p in range(pieces):
        for way in (-1, 1):
            @pl.when((place + way >= 0) & (place + way < sp_count))
            def _():
                line_go(real(place + way), z, p).start()
    turn(1, 0)
    route(z)
    lax.fori_loop(1, sp_count, route_other, 0)

    def out_copy(q):
        cols = pl.ds(q * piece, piece)
        return pltpu.make_async_copy(result.at[:, cols], out.at[:, cols], out_sem.at[q])

    def program(m):
        inner, outer = flip, 1 - flip

        def land(s, q):
            line_go(real(s), real(s), q).wait_recv()

        def send_in(s, q):
            line_go(real(m + 1), real(s), q).start()

        def send_out(s, q):
            line_go(real(m - 1), real(s), q).start()

        def pick(s, q):
            r = real(s)
            chosen = dot(slots[r], tokens[r, q]).astype(BF16)
            outbox[r, q] = chosen.reshape(tp_count, capacity, piece)
            for to in peers:
                go_copy(r, q, to, t).start()
            arrived[r, q, t] = outbox[r, q, t]

        def expert(s, _):
            r = real(s)
            gated = raised = None
            for q in range(pieces):
                box_wait(arrived, go_send, go_recv, r, q)
                block = arrived[r, q].reshape(picks, piece)
                part = slice(q * piece, (q + 1) * piece)
                a, b = dot(block, gate_w[part, :]), dot(block, up_w[part, :])
                gated, raised = (a, b) if q == 0 else (gated + a, raised + b)
            hidden = (gated / (1.0 + jnp.exp(-gated)) * raised).astype(BF16)
            for q in range(pieces):
                done = dot(hidden, down_w[:, q * piece : (q + 1) * piece]).astype(BF16)
                results[r, q] = done.reshape(tp_count, capacity, piece)
                if s != m:
                    give_back(s, q)
                returned[r, q, t] = results[r, q, t]

        def give_back(s, q):
            for to in peers:
                back_copy(real(s), q, to, t).start()

        def mix(s, q):
            r = real(s)
            box_wait(returned, back_send, back_recv, r, q)
            both = dot(shares[r], returned[r, q].reshape(picks, piece))
            mixed = both[:rows] + both[rows:]
            if s == m:
                total_own[q] = stream[:, q * piece : (q + 1) * piece].astype(F32) + mixed
            elif m == 0:
                line_out[r, q] = mixed.astype(BF16)
                line_back(real(1), r, q, inner).start()
            else:
                local[r, q] = mixed

        def hand_on(s, q):
            r = real(s)
            way, to = (inner, m + 1) if s > m else (outer, m - 1)
            line_back(real(to), r, q, way).wait_recv()
            line_out[r, q] = (local[r, q] + line_in[way, r, q].astype(F32)).astype(BF16)
            line_back(real(to), r, q, way).start()

        act = {
            "close": lambda *_: close(1), "send_in": send_in, "send_out": send_out,
            "pick": pick, "expert": expert, "back": give_back, "mix": mix, "pass": hand_on,
        }
        waited = set()
        for name, s, q in steps[m]:
            if name == "expert" and "loads" not in waited:
                waited.add("loads")
                for load in loads[3:]:
                    load.wait()
            for p in range(q, halves * pieces, pieces) if name == "pick" else [q]:
                if name in ("pick", "send_in", "send_out") and s != m and (s, p) not in waited:
                    waited.add((s, p))
                    land(s, p)
            act[name](s, q)
        for q in range(pieces):
            total = total_own[q]
            for way in [inner, outer] if m > 0 else [outer]:
                line_back(real(m + 1), z, q, way).wait_recv()
                total = total + line_in[way, z, q].astype(F32)
            result[:, q * piece : (q + 1) * piece] = total.astype(BF16)
            out_copy(q).start()
        peer = {"sp": real(m + 1)}
        for _ in range(sp_count + 1 if m > 0 else 1):
            sent(tokens.at[0], line_go_send, peer)
        sent(line_out.at[pl.ds(0, sp_count - 1)], line_back_send, peer)

    steps = timeline(sp_count, pieces, halves)
    for m in range((sp_count + 1) // 2):
        pl.when(place == m)(functools.partial(program, m))

    @pl.when(z < sp_count - 1)
    def _():
        halo_copy.wait_send()

    peer = {"tp": x * 2 + other}
    sent(facts.at[pl.ds(0, sp_count - 1)], facts_send, {"sp": (z + 1) % sp_count})
    sent(pair_out, pair_send, peer)
    sent(far_out, far_send, peer)
    sent(outbox.at[:, :, pl.ds(0, tp_count - 1)], go_send, peer)
    sent(results.at[:, :, pl.ds(0, tp_count - 1)], back_send, peer)
    for q in range(pieces):
        out_copy(q).wait()


def fused(
    queries, key_heads, value_heads, sink_logit, out_weight, residual, norm_gain, expert_ids, route_weights,
    gate_weight, up_weight, down_weight,
):
    rows, width = residual.shape
    sp_count, tp_count = lax.axis_size("sp"), lax.axis_size("tp")
    experts = sp_count * tp_count
    top_k = expert_ids.shape[1]
    capacity = max(2, 2 * top_k * rows // experts)
    hidden = gate_weight.shape[2]
    depth = out_weight.shape[0]
    pieces, halves = 4, 2
    chips = tp_count // 2
    piece = width // pieces
    part = (halves, chips, pieces, rows // halves, piece)
    line = (sp_count, pieces, rows, piece)
    box = (sp_count, pieces, tp_count, capacity, piece)
    picks = tp_count * capacity
    reach, groups, size = key_heads.shape
    keys, values = key_heads.transpose(1, 2, 0), value_heads.transpose(1, 2, 0)
    vmem = pl.BlockSpec(memory_space=pltpu.VMEM)
    hbm = pl.BlockSpec(memory_space=pl.ANY)
    dma = pltpu.SemaphoreType.DMA
    return pl.pallas_call(
        functools.partial(tail_kernel, (sp_count, tp_count, pieces, halves, capacity)),
        out_shape=jax.ShapeDtypeStruct((rows, width), BF16),
        in_specs=[hbm, vmem, vmem, vmem, hbm, hbm, vmem, vmem, vmem, hbm, hbm, hbm],
        out_specs=hbm,
        scratch_shapes=[
            pltpu.VMEM(queries.shape, BF16),
            pltpu.VMEM(residual.shape, BF16),
            pltpu.VMEM((WINDOW + reach, groups * 2 * size), BF16),
            pltpu.VMEM(queries.shape, BF16),
            dma,
            dma,
            pltpu.VMEM((depth, width), BF16),
            pltpu.VMEM((width, hidden), BF16),
            pltpu.VMEM((width, hidden), BF16),
            pltpu.VMEM((hidden, width), BF16),
            pltpu.VMEM(part, BF16),
            pltpu.VMEM(part, BF16),
            pltpu.VMEM(part[:1] + part[2:], BF16),
            pltpu.VMEM(part[:1] + part[2:], BF16),
            pltpu.VMEM(part, F32),
            pltpu.VMEM((rows, width), BF16),
            pltpu.VMEM((sp_count, 2 * top_k + -2 * top_k % 8, rows), F32),
            pltpu.VMEM((sp_count, picks, rows), BF16),
            pltpu.VMEM((sp_count, 2 * rows, picks), BF16),
            pltpu.VMEM(line, BF16),
            pltpu.VMEM(box, BF16),
            pltpu.VMEM(box, BF16),
            pltpu.VMEM(box, BF16),
            pltpu.VMEM(box, BF16),
            pltpu.VMEM(line, F32),
            pltpu.VMEM(line[1:], F32),
            pltpu.VMEM(line, BF16),
            pltpu.VMEM((2,) + line, BF16),
            pltpu.VMEM((rows, width), BF16),
            dma((6,)),
            dma((pieces,)),
            dma,
            dma((halves, chips, pieces)),
            dma,
            dma((halves, pieces)),
            dma,
            dma((sp_count,)),
            dma,
            dma((sp_count, halves * pieces)),
            dma,
            dma((sp_count, pieces)),
            dma,
            dma((sp_count, pieces)),
            dma,
            dma((2, sp_count, pieces)),
        ],
        compiler_params=pltpu.CompilerParams(
            collective_id=0, has_side_effects=True, vmem_limit_bytes=VMEM_BUDGET
        ),
    )(
        queries, keys, values, sink_logit[None], out_weight, residual, norm_gain[None], expert_ids.T, route_weights.T,
        gate_weight, up_weight, down_weight,
    )


def on_device(queries, key_heads, value_heads, sink_logit, *rest):
    rows_dev = rest[1].shape[0]
    experts = lax.axis_size("sp") * lax.axis_size("tp")
    fits = 2 * rest[3].shape[1] * rows_dev // experts % 16 == 0 and rows_dev % WINDOW == 0
    fits = fits and lax.axis_size("sp") > 1 and lax.axis_size("tp") == 4
    if fits:
        return fused(queries, key_heads, value_heads, sink_logit, *rest)
    return tail_plain(attention(queries, key_heads, value_heads, sink_logit), *rest)


def solution(mesh):
    return jax.shard_map(
        on_device,
        mesh=mesh,
        in_specs=(
            P(("grp", "sp"), "tp"),
            P(("grp", "sp"), "tp", None),
            P(("grp", "sp"), "tp", None),
            P("tp"),
            P("tp", None),
            P(("grp", "sp", "tp"), None),
            P(),
            P(("grp", "sp", "tp"), None),
            P(("grp", "sp", "tp"), None),
            P(("sp", "tp"), None, None),
            P(("sp", "tp"), None, None),
            P(("sp", "tp"), None, None),
        ),
        out_specs=P(("grp", "sp", "tp"), None),
        check_vma=False,
    )
```

```python
import functools

import jax
import jax.numpy as jnp
from jax import lax
from jax.experimental import pallas as pl
from jax.experimental.pallas import tpu as pltpu
from jax.sharding import PartitionSpec as P

WINDOW = 128


EPS = 1e-06

F32 = jnp.float32
BF16 = jnp.bfloat16
MESH = pl.DeviceIdType.MESH
VMEM_BUDGET = 54 * 1024 * 1024


def from_behind(value, axis, steps):
    count = lax.axis_size(axis)
    initial, last = (max(0, -steps), min(count, count - steps))
    return lax.ppermute(value, axis, [(source, source + steps) for source in range(initial, last)])


def dot(a, b, dims=((1,), (0,))):
    return lax.dot_general(a, b, (dims, ((), ())), preferred_element_type=F32)


def attention(queries, key_heads, value_heads, sink_logit):
    rows_sp = queries.shape[0]
    kv_local = key_heads.shape[1]
    head_dim = key_heads.shape[2]
    heads_local = queries.shape[1] // head_dim
    group_size = heads_local // kv_local
    window = WINDOW
    count_of_blocks = rows_sp // window
    edge = jnp.stack([key_heads[rows_sp - window :], value_heads[rows_sp - window :]])
    tail_rows = from_behind(edge, "sp", 1)
    key_blocks = jnp.concatenate([tail_rows[0], key_heads], 0).reshape(
        count_of_blocks + 1, window, kv_local, head_dim
    )
    value_blocks = jnp.concatenate([tail_rows[1], value_heads], 0).reshape(
        count_of_blocks + 1, window, kv_local, head_dim
    )
    key_span = jnp.concatenate([key_blocks[:-1], key_blocks[1:]], 1)
    value_span = jnp.concatenate([value_blocks[:-1], value_blocks[1:]], 1)
    query_pos = jnp.arange(window, dtype=jnp.int32)[:, None]
    key_pos = jnp.arange(2 * window, dtype=jnp.int32)[None, :]
    distance = query_pos + window - key_pos
    band = (distance >= 0) & (distance < window)
    key_start = (
        lax.axis_index("sp") * rows_sp
        + jnp.arange(count_of_blocks, dtype=jnp.int32)[:, None] * window
        - window
        + key_pos
    )
    allowed = band[None, :, :] & (key_start >= 0)[:, None, :]
    query_blocks = queries.reshape(count_of_blocks, window, kv_local, group_size, head_dim)
    logit_scores = jnp.einsum(
        "bqhgd,bkhd->bhgqk", query_blocks, key_span, preferred_element_type=jnp.float32
    ) * head_dim ** (-0.5)
    logit_scores = jnp.where(allowed[:, None, None], logit_scores, -jnp.inf)
    sink_col = sink_logit.reshape(kv_local, group_size)[None, :, :, None, None]
    row_max = jnp.maximum(jnp.max(logit_scores, axis=-1, keepdims=True), sink_col)
    expd = jnp.exp(logit_scores - row_max)
    row_total = jnp.sum(expd, axis=-1, keepdims=True) + jnp.exp(sink_col - row_max)
    attention_probabilities = (expd / row_total).astype(jnp.bfloat16)
    attended = jnp.einsum(
        "bhgqk,bkhd->bqhgd", attention_probabilities, value_span, preferred_element_type=jnp.float32
    ).astype(jnp.bfloat16)
    return attended.reshape(rows_sp, heads_local * head_dim)


def tail_plain(
    attended, out_weight, residual, norm_gain, expert_ids, route_weights,
    gate_weight, up_weight, down_weight,
):
    rows_dev = residual.shape[0]
    width = residual.shape[1]
    projected = lax.psum_scatter(
        jnp.dot(attended, out_weight, preferred_element_type=jnp.float32),
        "tp",
        scatter_dimension=0,
        tiled=True,
    )
    stream = (residual.astype(jnp.float32) + projected).astype(jnp.bfloat16)
    wide = stream.astype(jnp.float32)
    normed = (
        wide * lax.rsqrt(jnp.mean(wide * wide, axis=-1, keepdims=True) + EPS) * norm_gain
    ).astype(jnp.bfloat16)
    sp_count = lax.axis_size("sp")
    tp_count = lax.axis_size("tp")
    experts_total = sp_count * tp_count
    top_k = expert_ids.shape[1]
    capacity = max(2, 2 * top_k * rows_dev // experts_total)
    flat_ids = expert_ids.reshape(-1)
    pairs = flat_ids.shape[0]
    onehot = (flat_ids[:, None] == jnp.arange(experts_total, dtype=jnp.int32)[None, :]).astype(
        jnp.int32
    )
    earlier = jnp.cumsum(onehot, axis=0) - onehot
    slot_rank = jnp.sum(earlier * onehot, axis=1)
    flat_slot = flat_ids * capacity + slot_rank
    owner_row = jnp.arange(pairs, dtype=jnp.int32) // top_k
    token_in_slot = jnp.zeros((experts_total * capacity,), jnp.int32).at[flat_slot].set(owner_row)
    filled = jnp.zeros((experts_total * capacity,), jnp.bool_).at[flat_slot].set(True)
    outbox = jnp.where(filled[:, None], normed[token_in_slot], jnp.zeros((), jnp.bfloat16))
    outbox = outbox.reshape(experts_total, capacity, width)
    arrived = lax.all_to_all(outbox, ("sp", "tp"), split_axis=0, concat_axis=0, tiled=True)
    rows = arrived.reshape(-1, width)
    gate = jnp.dot(rows, gate_weight[0], preferred_element_type=jnp.float32)
    upward = jnp.dot(rows, up_weight[0], preferred_element_type=jnp.float32)
    expert_hidden = (jax.nn.silu(gate) * upward).astype(jnp.bfloat16)
    expert_rows = jnp.dot(expert_hidden, down_weight[0], preferred_element_type=jnp.float32).astype(
        jnp.bfloat16
    )
    results = expert_rows.reshape(arrived.shape)
    returned = lax.all_to_all(results, ("sp", "tp"), split_axis=0, concat_axis=0, tiled=True)
    picked_rows = returned.reshape(experts_total * capacity, width)[flat_slot].reshape(
        rows_dev, top_k, width
    )
    shares = route_weights / jnp.sum(route_weights, axis=-1, keepdims=True)
    combined = jnp.sum(shares[:, :, None] * picked_rows.astype(jnp.float32), axis=1)
    return (wide + combined).astype(jnp.bfloat16)


def routing(facts, first, top_k, experts, capacity):
    facts = facts.T
    rows = facts.shape[0]
    ids, weights = facts[:, :top_k], facts[:, top_k : 2 * top_k]
    expert = (first + lax.broadcasted_iota(jnp.int32, (rows, experts), 1)).astype(F32)
    total = jnp.sum(weights, axis=1, keepdims=True)
    member = jnp.zeros((rows, experts), F32)
    share = jnp.zeros((rows, experts), F32)
    for k in range(top_k):
        hit = jnp.where(ids[:, k : k + 1] == expert, 1.0, 0.0)
        member = member + hit
        share = share + hit * (weights[:, k : k + 1] / total)
    before = (
        lax.broadcasted_iota(jnp.int32, (rows, rows), 0)
        > lax.broadcasted_iota(jnp.int32, (rows, rows), 1)
    ).astype(BF16)
    rank = dot(before, member.astype(BF16))
    rank = jnp.where(member > 0, rank, -1.0)
    slots = experts * capacity
    spread = (
        lax.broadcasted_iota(jnp.int32, (experts, slots), 1) // capacity
        == lax.broadcasted_iota(jnp.int32, (experts, slots), 0)
    ).astype(BF16)
    rank_slot = dot(rank.astype(BF16), spread)
    place = lax.broadcasted_iota(jnp.int32, (rows, slots), 1) % capacity
    taken = rank_slot == place.astype(F32)
    high = share.astype(BF16)
    low = (share - high.astype(F32)).astype(BF16)
    one = jnp.where(taken, 1.0, 0.0)
    shares = jnp.concatenate([one * dot(high, spread), one * dot(low, spread)], 0)
    return one.T.astype(BF16), shares.astype(BF16)


def attend(z, queries, sink, seen, attended, first, count):
    window = WINDOW
    rows, lanes = queries.shape[0], seen.shape[1]
    heads = sink.shape[1]
    size = queries.shape[1] // heads
    groups = lanes // (2 * size)
    share = heads // groups
    pairs = share // 2
    tall, reach = pairs * count, window + count
    query = lax.broadcasted_iota(jnp.int32, (tall, reach), 0) % count
    key = lax.broadcasted_iota(jnp.int32, (tall, reach), 1)
    distance = query + window - key
    allowed = (distance >= 0) & (distance < window) & ((z * rows + first - window) + key >= 0)
    span = seen[pl.ds(pl.multiple_of(first, count), reach), :]
    here = pl.ds(pl.multiple_of(first, count), count)
    for g in range(groups):
        keys = span[:, 2 * g * size : (2 * g + 1) * size]
        values = span[:, (2 * g + 1) * size : (2 * g + 2) * size]
        none, ones = jnp.zeros_like(keys), jnp.ones_like(values)
        wide = jnp.concatenate(
            [
                queries[here, (g * share + 2 * i) * size : (g * share + 2 * i + 2) * size]
                for i in range(pairs)
            ],
            0,
        )
        sides = []
        for odd in range(2):
            two_keys = jnp.concatenate([none, keys] if odd else [keys, none], 1)
            two_values = jnp.concatenate([ones, values] if odd else [values, ones], 1)
            score = dot(wide, two_keys, ((1,), (1,))) * size**-0.5
            score = jnp.where(allowed, score, -1e30)
            drain = jnp.concatenate(
                [
                    jnp.broadcast_to(
                        sink[0:1, g * share + 2 * i + odd : g * share + 2 * i + odd + 1],
                        (count, 1),
                    )
                    for i in range(pairs)
                ],
                0,
            )
            top = jnp.maximum(jnp.max(score, axis=1, keepdims=True), drain)
            grown = jnp.exp(score - top).astype(BF16)
            both = dot(grown, two_values)
            at = 0 if odd else size
            total = both[:, at : at + 1] + jnp.exp(drain - top)
            sides.append(both * (1.0 / total))
        lane = lax.broadcasted_iota(jnp.int32, (tall, 2 * size), 1)
        both = jnp.where(lane < size, sides[0], sides[1]).astype(BF16)
        for i in range(pairs):
            at = (g * share + 2 * i) * size
            attended[here, at : at + 2 * size] = both[i * count : (i + 1) * count]


def timeline(count, pieces, halves, favour=None):
    hop, narrow, tick = 0.7, 0.5, 0.05
    line_lead, layer_lead, begun, spare = 0.3, 0.3, 1.9, 0.3
    cost = {"close": 0.2, "pick": 0.07, "expert": 0.67, "mix": 0.08, "pass": 0.02}
    every = range(count)
    bits = [(s, p) for s in every for p in range(halves * pieces)]
    parts = [(s, q) for s in every for q in range(pieces)]
    landed, came, worked, back, mixed, handed = {}, {}, {}, {}, {}, {}
    line, layer, busy = {}, [1.1] * count, [begun] * count
    done = [set() for _ in every]
    steps = [[] for _ in every]
    now = 0.0

    def put(d, way, at, board, part, size):
        line[d, way] = max(line.get((d, way), 0.0), at) + size
        key = (d + way,) + part
        board[key] = max(board.get(key, 0.0), line[d, way] + hop)

    def there(board, d, part):
        return board.get((d,) + part, now + 1) <= now

    def whole(d, p):
        return all(there(landed, d, (p[0], h * pieces + p[1])) for h in range(halves))

    def choose(d):
        for way, name in ((-1, "send_out"), (1, "send_in")):
            if 0 <= d + way < count and line.get((d, way), 0.0) <= now + line_lead:
                ready = [
                    p
                    for p in bits
                    if (p[0] - d) * way <= 0 and there(landed, d, p) and (name, p) not in done[d]
                ]
                if ready:
                    end = d + way in (0, count - 1)
                    return name, min(ready, key=lambda p: (end and p[0] == d, abs(p[0] - d), p[1]))
        if ("close", (d, 0)) not in done[d]:
            return "close", (d, 0)
        ready = [
            p
            for p in parts
            if p[0] != d and there(handed, d, p) and there(mixed, d, p) and ("pass", p) not in done[d]
        ]
        if ready:
            return "pass", min(ready, key=lambda p: handed[(d,) + p])
        for p in parts:
            if there(back, d, p) and ("mix", p) not in done[d]:
                return "mix", p
        ready = [
            (s, 0)
            for s in every
            if there(came, d, (s, pieces - 1)) and ("expert", (s, 0)) not in done[d]
        ]
        if ready:
            return "expert", min(ready, key=lambda p: came[d, p[0], pieces - 1])
        ready = [p for p in parts if whole(d, p) and ("pick", p) not in done[d]]
        if ready and layer[d] <= now + layer_lead:
            return "pick", min(ready, key=lambda p: (favour[d][p[0]] if favour else 0, p))
        ready = [p for p in parts if p[0] == d and there(worked, d, p) and ("back", p) not in done[d]]
        if ready and layer[d] <= now:
            return "back", ready[0]
        return None

    for d in every:
        for p in range(pieces):
            landed[d, d, p] = 0.0
            for way, name in ((-1, "send_out"), (1, "send_in")):
                if 0 <= d + way < count:
                    put(d, way, 0.0, landed, (d, p), 1 / halves)
                    done[d].add((name, (d, p)))
    size = count * pieces
    due = [{"mix": size, "pass": size - pieces if 0 < d < count - 1 else 0} for d in every]
    while any(sum(k == name for k, _ in done[d]) < due[d][name] for d in every for name in due[d]):
        for d in every:
            while busy[d] <= now:
                step = choose(d)
                if step is None:
                    break
                name, part = step
                done[d].add(step)
                steps[d].append((name,) + part)
                busy[d] = now + cost.get(name, 0.0)
                if name == "send_in":
                    put(d, 1, now, landed, part, 1 / halves)
                elif name == "send_out":
                    put(d, -1, now, landed, part, 1 / halves)
                elif name == "close":
                    for p in range(pieces, halves * pieces):
                        landed[d, d, p] = busy[d]
                elif name == "pick":
                    layer[d] = max(layer[d], busy[d]) + narrow
                    came[(d,) + part] = layer[d] + hop + (spare if 0 < d < count - 1 else 0)
                elif name == "expert":
                    for q in range(pieces):
                        if part[0] == d:
                            worked[d, d, q] = busy[d]
                            continue
                        ready = now + cost[name] * (q + 3) / (pieces + 2)
                        layer[d] = max(layer[d], ready) + narrow
                        back[d, part[0], q] = layer[d] + hop
                elif name == "back":
                    layer[d] = max(layer[d], now) + narrow
                    back[(d,) + part] = layer[d] + hop
                elif name == "mix":
                    mixed[(d,) + part] = busy[d]
                if name == "pass" or (name == "mix" and part[0] != d and d in (0, count - 1)):
                    put(d, 1 if part[0] > d else -1, busy[d], handed, part, 1)
        now += tick
    if favour is None:
        ends = [[landed[d, s, halves * pieces - 1] for s in every] for d in every]
        return timeline(count, pieces, halves, ends)
    return steps


def tail_kernel(
    sizes,
    queries_hbm, keys_hbm, values_hbm, sink_hbm, out_w_hbm, residual_hbm, gain_hbm, ids_hbm, weights_hbm,
    gate_hbm, up_hbm, down_hbm,
    out,
    queries, keys, values, sink, residual, gain, ids, weights, seen, attended, halo_send, halo_recv,
    out_w, gate_w, up_w, down_w,
    pair_out, pair_in, far_out, far_in, mine,
    stream, facts, slots, shares,
    tokens, outbox, arrived, results, returned,
    local, total_own, line_out, line_in,
    load_sem, pair_send, pair_recv, far_send, far_recv,
    facts_send, facts_recv, line_go_send, line_go_recv,
    go_send, go_recv, back_send, back_recv, line_back_send, line_back_recv,
):
    sp_count, tp_count, pieces, halves, capacity = sizes
    chips = tp_count // 2
    z, t = lax.axis_index("sp"), lax.axis_index("tp")
    x, core = t // 2, t % 2
    other = 1 - core
    rows, width = residual_hbm.shape
    piece, half = width // pieces, rows // halves
    top_k = ids_hbm.shape[0]
    picks = tp_count * capacity

    barrier = pltpu.get_barrier_semaphore()
    for k in range(1, sp_count):
        pl.semaphore_signal(
            barrier, inc=1, device_id={"sp": (z + k) % sp_count}, device_id_type=MESH
        )
    for k in range(1, tp_count):
        pl.semaphore_signal(
            barrier, inc=1, device_id={"tp": (t + k) % tp_count}, device_id_type=MESH
        )
    loads = [
        pltpu.make_async_copy(src, dst, load_sem.at[i])
        for i, (src, dst) in enumerate(
            (
                (keys_hbm, keys), (values_hbm, values), (queries_hbm, queries), (sink_hbm, sink),
                (ids_hbm, ids), (weights_hbm, weights), (out_w_hbm, out_w), (residual_hbm, residual),
                (gain_hbm, gain), (gate_hbm.at[0], gate_w), (up_hbm.at[0], up_w), (down_hbm.at[0], down_w),
            )
        )
    ]
    for load in loads:
        load.start()

    groups, size, reach = keys.shape
    for load in loads[:2]:
        load.wait()
    for g in range(groups):
        both = jnp.concatenate([keys[g], values[g]], 0)
        seen[WINDOW:, 2 * g * size : (2 * g + 2) * size] = both.T

    @pl.when(z == 0)
    def _():
        seen[:WINDOW, :] = jnp.zeros((WINDOW, seen.shape[1]), BF16)

    for load in loads[2:6]:
        load.wait()
    pad = jnp.zeros((-2 * top_k % 8, rows), F32)
    facts[z] = jnp.concatenate([ids[...].astype(F32), weights[...], pad], 0)
    def facts_copy(k):
        return pltpu.make_async_remote_copy(
            facts.at[z], facts.at[z], facts_send, facts_recv.at[z],
            device_id={"sp": (z + k) % sp_count}, device_id_type=MESH,
        )

    def facts_wait(s):
        pltpu.make_async_remote_copy(
            facts.at[s], facts.at[s], facts_send, facts_recv.at[s],
            device_id={"sp": s}, device_id_type=MESH,
        ).wait_recv()

    def route(s):
        slots[s], shares[s] = routing(facts[s], z * tp_count, top_k, tp_count, capacity)

    halo_copy = pltpu.make_async_remote_copy(
        seen.at[pl.ds(reach, WINDOW)], seen.at[pl.ds(0, WINDOW)], halo_send, halo_recv,
        device_id={"sp": jnp.minimum(z + 1, sp_count - 1)}, device_id_type=MESH,
    )

    def attend_half(at, h):
        attend(z, queries, sink, seen, attended, at * rows + h * half, half)

    def pair_copy(h, k, q):
        return pltpu.make_async_remote_copy(
            pair_out.at[h, k, q], pair_in.at[h, k, q], pair_send, pair_recv.at[h, k, q],
            device_id={"tp": x * 2 + other}, device_id_type=MESH,
        )

    def far_copy(h, q):
        return pltpu.make_async_remote_copy(
            far_out.at[h, q], far_in.at[h, q], far_send, far_recv.at[h, q],
            device_id={"tp": (1 - x) * 2 + core}, device_id_type=MESH,
        )

    def far_out_all(h):
        for q in range(pieces):
            pair_copy(h, 1, q).wait_recv()
            far_out[h, q] = (mine[h, 1, q] + pair_in[h, 1, q].astype(F32)).astype(BF16)
            far_copy(h, q).start()

    def taken(at, h):
        return attended[pl.ds(pl.multiple_of(at * rows + h * half, half), half), :]

    def give(h, k):
        chip = (x + k) % chips
        block = jnp.concatenate([taken(chip * 2 + other, h), taken(chip * 2 + core, h)], 0)
        for q in range(pieces):
            both = dot(block, out_w[:, q * piece : (q + 1) * piece])
            pair_out[h, k, q] = both[:half].astype(BF16)
            pair_copy(h, k, q).start()
            mine[h, k, q] = both[half:]
        if k:
            far_out_all(h)

    def give_one(h, at):
        block = taken(at, h)
        for q in range(pieces):
            one = dot(block, out_w[:, q * piece : (q + 1) * piece])

            @pl.when(at % 2 == core)
            def _():
                mine[h, 1, q] = one

            @pl.when(at % 2 == other)
            def _():
                pair_out[h, 1, q] = one.astype(BF16)
                pair_copy(h, 1, q).start()

        @pl.when(at % 2 == core)
        def _():
            far_out_all(h)

    def first_rows():
        @pl.when(z > 0)
        def _():
            halo_copy.wait_recv()

        attend_half(0, 0)

    def turn(h, k):
        chip = (x + k) % chips
        attend_half(chip * 2 + 1, h)
        attend_half(chip * 2, h)
        give(h, k)

    def close(h):
        here = slice(h * half, (h + 1) * half)
        square = jnp.zeros((half, 1), F32)
        for q in range(pieces):
            cols = slice(q * piece, (q + 1) * piece)
            total = mine[h, 0, q]
            pair_copy(h, 0, q).wait_recv()
            total = total + pair_in[h, 0, q].astype(F32)
            far_copy(h, q).wait_recv()
            total = total + far_in[h, q].astype(F32)
            value = (residual[here, cols].astype(F32) + total).astype(BF16)
            stream[here, cols] = value
            value = value.astype(F32)
            square = square + jnp.sum(value * value, axis=1, keepdims=True)
        scale = lax.rsqrt(square / width + EPS)
        for q in range(pieces):
            cols = slice(q * piece, (q + 1) * piece)
            tokens[z, q, here, :] = (stream[here, cols].astype(F32) * scale * gain[:, cols]).astype(BF16)

    def route_other(k, carry):
        s = (z + k) % sp_count
        facts_wait(s)
        route(s)
        return carry

    def line_go(to, s, p):
        bit = tokens.at[s, p % pieces, pl.ds(p // pieces * half, half)]
        return pltpu.make_async_remote_copy(
            bit, bit, line_go_send, line_go_recv.at[s, p],
            device_id={"sp": to}, device_id_type=MESH,
        )

    def line_back(to, s, q, way, last=False):
        return pltpu.make_async_remote_copy(
            line_out.at[s, q], line_in.at[way, s, q], line_back_send,
            line_back_recv.at[s + last * way * (sp_count - s), q], device_id={"sp": to}, device_id_type=MESH,
        )

    def go_copy(s, q, to, at):
        return pltpu.make_async_remote_copy(
            outbox.at[s, q, to], arrived.at[s, q, at], go_send, go_recv.at[s, q],
            device_id={"tp": to}, device_id_type=MESH,
        )

    def back_copy(s, q, to, at):
        return pltpu.make_async_remote_copy(
            results.at[s, q, to], returned.at[s, q, at], back_send, back_recv.at[s, q],
            device_id={"tp": to}, device_id_type=MESH,
        )

    def box_wait(box, send, recv, s, q):
        part = pl.ds(0, tp_count - 1)
        pltpu.make_async_remote_copy(
            box.at[s, q, part], box.at[s, q, part], send, recv.at[s, q],
            device_id={"tp": (t + 1) % tp_count}, device_id_type=MESH,
        ).wait_recv()

    def sent(ref, send, peer):
        pltpu.make_async_remote_copy(
            ref, ref, send, halo_recv, device_id=peer, device_id_type=MESH
        ).wait_send()

    peers = [(t + k) % tp_count for k in range(1, tp_count)]
    flip = (z * 2 >= sp_count).astype(jnp.int32)
    place = z + flip * (sp_count - 1 - 2 * z)

    def real(s):
        return s + flip * (sp_count - 1 - 2 * s)

    attend_half((chips - 1) * 2 + 1, 0)
    attend_half((chips - 1) * 2, 0)
    pl.semaphore_wait(barrier, sp_count + tp_count - 2)

    @pl.when(z < sp_count - 1)
    def _():
        halo_copy.start()

    for k in range(1, sp_count):
        facts_copy(k).start()
    loads[6].wait()

    @pl.when(x == 0)
    def _():
        give(0, 1)

    @pl.when(x == 1)
    def _():
        attend_half(1, 0)
        give_one(0, 1)
        first_rows()
        give_one(0, 0)

    turn(1, 1)

    @pl.when(x == 0)
    def _():
        attend_half(1, 0)
        first_rows()

    give(0, 0)
    for load in loads[7:9]:
        load.wait()
    close(0)
    for p in range(pieces):
        for way in (-1, 1):
            @pl.when((place + way >= 0) & (place + way < sp_count))
            def _():
                line_go(real(place + way), z, p).start()
    turn(1, 0)
    route(z)
    lax.fori_loop(1, sp_count, route_other, 0)

    def program(m):
        inner, outer = flip, 1 - flip

        def land(s, q):
            line_go(real(s), real(s), q).wait_recv()

        def send_in(s, q):
            line_go(real(m + 1), real(s), q).start()

        def send_out(s, q):
            line_go(real(m - 1), real(s), q).start()

        def pick(s, q):
            r = real(s)
            chosen = dot(slots[r], tokens[r, q]).astype(BF16)
            outbox[r, q] = chosen.reshape(tp_count, capacity, piece)
            for to in peers:
                go_copy(r, q, to, t).start()
            arrived[r, q, t] = outbox[r, q, t]

        def expert(s, _):
            r = real(s)
            gated = raised = None
            for q in range(pieces):
                box_wait(arrived, go_send, go_recv, r, q)
                block = arrived[r, q].reshape(picks, piece)
                part = slice(q * piece, (q + 1) * piece)
                a, b = dot(block, gate_w[part, :]), dot(block, up_w[part, :])
                gated, raised = (a, b) if q == 0 else (gated + a, raised + b)
            hidden = (gated / (1.0 + jnp.exp(-gated)) * raised).astype(BF16)
            for q in range(pieces):
                done = dot(hidden, down_w[:, q * piece : (q + 1) * piece]).astype(BF16)
                results[r, q] = done.reshape(tp_count, capacity, piece)
                if s != m:
                    give_back(s, q)
                returned[r, q, t] = results[r, q, t]

        def give_back(s, q):
            for to in peers:
                back_copy(real(s), q, to, t).start()

        def mix(s, q):
            r = real(s)
            box_wait(returned, back_send, back_recv, r, q)
            both = dot(shares[r], returned[r, q].reshape(picks, piece))
            mixed = both[:rows] + both[rows:]
            if s == m:
                total_own[q] = stream[:, q * piece : (q + 1) * piece].astype(F32) + mixed
            elif m == 0:
                line_out[r, q] = mixed.astype(BF16)
                line_back(real(1), r, q, inner, s == 1).start()
            else:
                local[r, q] = mixed

        def hand_on(s, q):
            r = real(s)
            way, to = (inner, m + 1) if s > m else (outer, m - 1)
            line_back(real(to), r, q, way).wait_recv()
            line_out[r, q] = (local[r, q] + line_in[way, r, q].astype(F32)).astype(BF16)
            line_back(real(to), r, q, way, s == to).start()

        act = {
            "close": lambda *_: close(1), "send_in": send_in, "send_out": send_out,
            "pick": pick, "expert": expert, "back": give_back, "mix": mix, "pass": hand_on,
        }
        waited = set()
        for name, s, q in steps[m]:
            if name == "expert" and "loads" not in waited:
                waited.add("loads")
                for load in loads[9:]:
                    load.wait()
            for p in range(q, halves * pieces, pieces) if name == "pick" else [q]:
                if name in ("pick", "send_in", "send_out") and s != m and (s, p) not in waited:
                    waited.add((s, p))
                    land(s, p)
            act[name](s, q)
        for q in range(pieces):
            total = total_own[q]
            for way in [inner, outer] if m > 0 else [outer]:
                line_back(real(m + 1), z, q, way, True).wait_recv()
                total = total + line_in[way, z, q].astype(F32)
            out[:, q * piece : (q + 1) * piece] = total.astype(BF16)
        peer = {"sp": real(m + 1)}
        for _ in range(sp_count + 1 if m > 0 else 1):
            sent(tokens.at[0], line_go_send, peer)
        sent(line_out.at[pl.ds(0, sp_count - 1)], line_back_send, peer)

    steps = timeline(sp_count, pieces, halves)
    for m in range((sp_count + 1) // 2):
        pl.when(place == m)(functools.partial(program, m))

    @pl.when(z < sp_count - 1)
    def _():
        halo_copy.wait_send()

    peer = {"tp": x * 2 + other}
    sent(facts.at[pl.ds(0, sp_count - 1)], facts_send, {"sp": (z + 1) % sp_count})
    sent(pair_out, pair_send, peer)
    sent(far_out, far_send, peer)
    sent(outbox.at[:, :, pl.ds(0, tp_count - 1)], go_send, peer)
    sent(results.at[:, :, pl.ds(0, tp_count - 1)], back_send, peer)


def fused(
    queries, key_heads, value_heads, sink_logit, out_weight, residual, norm_gain, expert_ids, route_weights,
    gate_weight, up_weight, down_weight,
):
    rows, width = residual.shape
    sp_count, tp_count = lax.axis_size("sp"), lax.axis_size("tp")
    experts = sp_count * tp_count
    top_k = expert_ids.shape[1]
    capacity = max(2, 2 * top_k * rows // experts)
    hidden = gate_weight.shape[2]
    depth = out_weight.shape[0]
    pieces, halves = 4, 2
    chips = tp_count // 2
    piece = width // pieces
    part = (halves, chips, pieces, rows // halves, piece)
    line = (sp_count, pieces, rows, piece)
    box = (sp_count, pieces, tp_count, capacity, piece)
    picks = tp_count * capacity
    reach, groups, size = key_heads.shape
    keys, values = key_heads.transpose(1, 2, 0), value_heads.transpose(1, 2, 0)
    vmem = pl.BlockSpec(memory_space=pltpu.VMEM)
    hbm = pl.BlockSpec(memory_space=pltpu.MemorySpace.HBM)
    dma = pltpu.SemaphoreType.DMA
    return pl.pallas_call(
        functools.partial(tail_kernel, (sp_count, tp_count, pieces, halves, capacity)),
        out_shape=pltpu.VMEM((rows, width), BF16),
        in_specs=[hbm] * 12,
        out_specs=vmem,
        scratch_shapes=[
            pltpu.VMEM(queries.shape, BF16),
            pltpu.VMEM(keys.shape, BF16),
            pltpu.VMEM(values.shape, BF16),
            pltpu.VMEM((1,) + sink_logit.shape, F32),
            pltpu.VMEM(residual.shape, BF16),
            pltpu.VMEM((1,) + norm_gain.shape, F32),
            pltpu.VMEM((top_k, rows), jnp.int32),
            pltpu.VMEM((top_k, rows), F32),
            pltpu.VMEM((WINDOW + reach, groups * 2 * size), BF16),
            pltpu.VMEM(queries.shape, BF16),
            dma,
            dma,
            pltpu.VMEM((depth, width), BF16),
            pltpu.VMEM((width, hidden), BF16),
            pltpu.VMEM((width, hidden), BF16),
            pltpu.VMEM((hidden, width), BF16),
            pltpu.VMEM(part, BF16),
            pltpu.VMEM(part, BF16),
            pltpu.VMEM(part[:1] + part[2:], BF16),
            pltpu.VMEM(part[:1] + part[2:], BF16),
            pltpu.VMEM(part, F32),
            pltpu.VMEM((rows, width), BF16),
            pltpu.VMEM((sp_count, 2 * top_k + -2 * top_k % 8, rows), F32),
            pltpu.VMEM((sp_count, picks, rows), BF16),
            pltpu.VMEM((sp_count, 2 * rows, picks), BF16),
            pltpu.VMEM(line, BF16),
            pltpu.VMEM(box, BF16),
            pltpu.VMEM(box, BF16),
            pltpu.VMEM(box, BF16),
            pltpu.VMEM(box, BF16),
            pltpu.VMEM(line, F32),
            pltpu.VMEM(line[1:], F32),
            pltpu.VMEM(line, BF16),
            pltpu.VMEM((2,) + line, BF16),
            dma((12,)),
            dma,
            dma((halves, chips, pieces)),
            dma,
            dma((halves, pieces)),
            dma,
            dma((sp_count,)),
            dma,
            dma((sp_count, halves * pieces)),
            dma,
            dma((sp_count, pieces)),
            dma,
            dma((sp_count, pieces)),
            dma,
            dma((sp_count + 1, pieces)),
        ],
        compiler_params=pltpu.CompilerParams(
            collective_id=0, has_side_effects=True, vmem_limit_bytes=VMEM_BUDGET
        ),
    )(
        queries, keys, values, sink_logit[None], out_weight, residual, norm_gain[None], expert_ids.T, route_weights.T,
        gate_weight, up_weight, down_weight,
    )


def on_device(queries, key_heads, value_heads, sink_logit, *rest):
    rows_dev = rest[1].shape[0]
    experts = lax.axis_size("sp") * lax.axis_size("tp")
    fits = 2 * rest[3].shape[1] * rows_dev // experts % 16 == 0 and rows_dev % WINDOW == 0
    fits = fits and lax.axis_size("sp") > 1 and lax.axis_size("tp") == 4
    if fits:
        return fused(queries, key_heads, value_heads, sink_logit, *rest)
    return tail_plain(attention(queries, key_heads, value_heads, sink_logit), *rest)


def solution(mesh):
    return jax.shard_map(
        on_device,
        mesh=mesh,
        in_specs=(
            P(("grp", "sp"), "tp"),
            P(("grp", "sp"), "tp", None),
            P(("grp", "sp"), "tp", None),
            P("tp"),
            P("tp", None),
            P(("grp", "sp", "tp"), None),
            P(),
            P(("grp", "sp", "tp"), None),
            P(("grp", "sp", "tp"), None),
            P(("sp", "tp"), None, None),
            P(("sp", "tp"), None, None),
            P(("sp", "tp"), None, None),
        ),
        out_specs=P(("grp", "sp", "tp"), None),
        check_vma=False,
    )
```

```python
import functools

import jax
import jax.numpy as jnp
from jax import lax
from jax.experimental import pallas as pl
from jax.experimental.pallas import tpu as pltpu
from jax.sharding import PartitionSpec as P

WINDOW = 128


EPS = 1e-06

F32 = jnp.float32
BF16 = jnp.bfloat16
MESH = pl.DeviceIdType.MESH
VMEM_BUDGET = 54 * 1024 * 1024


def from_behind(value, axis, steps):
    count = lax.axis_size(axis)
    initial, last = (max(0, -steps), min(count, count - steps))
    return lax.ppermute(value, axis, [(source, source + steps) for source in range(initial, last)])


def dot(a, b, dims=((1,), (0,))):
    return lax.dot_general(a, b, (dims, ((), ())), preferred_element_type=F32)


def attention(queries, key_heads, value_heads, sink_logit):
    rows_sp = queries.shape[0]
    kv_local = key_heads.shape[1]
    head_dim = key_heads.shape[2]
    heads_local = queries.shape[1] // head_dim
    group_size = heads_local // kv_local
    window = WINDOW
    count_of_blocks = rows_sp // window
    edge = jnp.stack([key_heads[rows_sp - window :], value_heads[rows_sp - window :]])
    tail_rows = from_behind(edge, "sp", 1)
    key_blocks = jnp.concatenate([tail_rows[0], key_heads], 0).reshape(
        count_of_blocks + 1, window, kv_local, head_dim
    )
    value_blocks = jnp.concatenate([tail_rows[1], value_heads], 0).reshape(
        count_of_blocks + 1, window, kv_local, head_dim
    )
    key_span = jnp.concatenate([key_blocks[:-1], key_blocks[1:]], 1)
    value_span = jnp.concatenate([value_blocks[:-1], value_blocks[1:]], 1)
    query_pos = jnp.arange(window, dtype=jnp.int32)[:, None]
    key_pos = jnp.arange(2 * window, dtype=jnp.int32)[None, :]
    distance = query_pos + window - key_pos
    band = (distance >= 0) & (distance < window)
    key_start = (
        lax.axis_index("sp") * rows_sp
        + jnp.arange(count_of_blocks, dtype=jnp.int32)[:, None] * window
        - window
        + key_pos
    )
    allowed = band[None, :, :] & (key_start >= 0)[:, None, :]
    query_blocks = queries.reshape(count_of_blocks, window, kv_local, group_size, head_dim)
    logit_scores = jnp.einsum(
        "bqhgd,bkhd->bhgqk", query_blocks, key_span, preferred_element_type=jnp.float32
    ) * head_dim ** (-0.5)
    logit_scores = jnp.where(allowed[:, None, None], logit_scores, -jnp.inf)
    sink_col = sink_logit.reshape(kv_local, group_size)[None, :, :, None, None]
    row_max = jnp.maximum(jnp.max(logit_scores, axis=-1, keepdims=True), sink_col)
    expd = jnp.exp(logit_scores - row_max)
    row_total = jnp.sum(expd, axis=-1, keepdims=True) + jnp.exp(sink_col - row_max)
    attention_probabilities = (expd / row_total).astype(jnp.bfloat16)
    attended = jnp.einsum(
        "bhgqk,bkhd->bqhgd", attention_probabilities, value_span, preferred_element_type=jnp.float32
    ).astype(jnp.bfloat16)
    return attended.reshape(rows_sp, heads_local * head_dim)


def tail_plain(
    attended, out_weight, residual, norm_gain, expert_ids, route_weights,
    gate_weight, up_weight, down_weight,
):
    rows_dev = residual.shape[0]
    width = residual.shape[1]
    projected = lax.psum_scatter(
        jnp.dot(attended, out_weight, preferred_element_type=jnp.float32),
        "tp",
        scatter_dimension=0,
        tiled=True,
    )
    stream = (residual.astype(jnp.float32) + projected).astype(jnp.bfloat16)
    wide = stream.astype(jnp.float32)
    normed = (
        wide * lax.rsqrt(jnp.mean(wide * wide, axis=-1, keepdims=True) + EPS) * norm_gain
    ).astype(jnp.bfloat16)
    sp_count = lax.axis_size("sp")
    tp_count = lax.axis_size("tp")
    experts_total = sp_count * tp_count
    top_k = expert_ids.shape[1]
    capacity = max(2, 2 * top_k * rows_dev // experts_total)
    flat_ids = expert_ids.reshape(-1)
    pairs = flat_ids.shape[0]
    onehot = (flat_ids[:, None] == jnp.arange(experts_total, dtype=jnp.int32)[None, :]).astype(
        jnp.int32
    )
    earlier = jnp.cumsum(onehot, axis=0) - onehot
    slot_rank = jnp.sum(earlier * onehot, axis=1)
    flat_slot = flat_ids * capacity + slot_rank
    owner_row = jnp.arange(pairs, dtype=jnp.int32) // top_k
    token_in_slot = jnp.zeros((experts_total * capacity,), jnp.int32).at[flat_slot].set(owner_row)
    filled = jnp.zeros((experts_total * capacity,), jnp.bool_).at[flat_slot].set(True)
    outbox = jnp.where(filled[:, None], normed[token_in_slot], jnp.zeros((), jnp.bfloat16))
    outbox = outbox.reshape(experts_total, capacity, width)
    arrived = lax.all_to_all(outbox, ("sp", "tp"), split_axis=0, concat_axis=0, tiled=True)
    rows = arrived.reshape(-1, width)
    gate = jnp.dot(rows, gate_weight[0], preferred_element_type=jnp.float32)
    upward = jnp.dot(rows, up_weight[0], preferred_element_type=jnp.float32)
    expert_hidden = (jax.nn.silu(gate) * upward).astype(jnp.bfloat16)
    expert_rows = jnp.dot(expert_hidden, down_weight[0], preferred_element_type=jnp.float32).astype(
        jnp.bfloat16
    )
    results = expert_rows.reshape(arrived.shape)
    returned = lax.all_to_all(results, ("sp", "tp"), split_axis=0, concat_axis=0, tiled=True)
    picked_rows = returned.reshape(experts_total * capacity, width)[flat_slot].reshape(
        rows_dev, top_k, width
    )
    shares = route_weights / jnp.sum(route_weights, axis=-1, keepdims=True)
    combined = jnp.sum(shares[:, :, None] * picked_rows.astype(jnp.float32), axis=1)
    return (wide + combined).astype(jnp.bfloat16)


def routing(facts, first, top_k, experts, capacity):
    facts = facts.T
    rows = facts.shape[0]
    ids, weights = facts[:, :top_k], facts[:, top_k : 2 * top_k]
    expert = (first + lax.broadcasted_iota(jnp.int32, (rows, experts), 1)).astype(F32)
    total = jnp.sum(weights, axis=1, keepdims=True)
    member = jnp.zeros((rows, experts), F32)
    share = jnp.zeros((rows, experts), F32)
    for k in range(top_k):
        hit = jnp.where(ids[:, k : k + 1] == expert, 1.0, 0.0)
        member = member + hit
        share = share + hit * (weights[:, k : k + 1] / total)
    before = (
        lax.broadcasted_iota(jnp.int32, (rows, rows), 0)
        > lax.broadcasted_iota(jnp.int32, (rows, rows), 1)
    ).astype(BF16)
    rank = dot(before, member.astype(BF16))
    rank = jnp.where(member > 0, rank, -1.0)
    slots = experts * capacity
    spread = (
        lax.broadcasted_iota(jnp.int32, (experts, slots), 1) // capacity
        == lax.broadcasted_iota(jnp.int32, (experts, slots), 0)
    ).astype(BF16)
    rank_slot = dot(rank.astype(BF16), spread)
    place = lax.broadcasted_iota(jnp.int32, (rows, slots), 1) % capacity
    taken = rank_slot == place.astype(F32)
    high = share.astype(BF16)
    low = (share - high.astype(F32)).astype(BF16)
    one = jnp.where(taken, 1.0, 0.0)
    shares = jnp.concatenate([one * dot(high, spread), one * dot(low, spread)], 0)
    return one.T.astype(BF16), shares.astype(BF16)


def attend(z, queries, sink, seen, attended, first, count):
    window = WINDOW
    rows, lanes = queries.shape[0], seen.shape[1]
    heads = sink.shape[1]
    size = queries.shape[1] // heads
    groups = lanes // (2 * size)
    share = heads // groups
    pairs = share // 2
    tall, reach = pairs * count, window + count
    query = lax.broadcasted_iota(jnp.int32, (tall, reach), 0) % count
    key = lax.broadcasted_iota(jnp.int32, (tall, reach), 1)
    distance = query + window - key
    allowed = (distance >= 0) & (distance < window) & ((z * rows + first - window) + key >= 0)
    span = seen[pl.ds(pl.multiple_of(first, count), reach), :]
    here = pl.ds(pl.multiple_of(first, count), count)
    for g in range(groups):
        keys = span[:, 2 * g * size : (2 * g + 1) * size]
        values = span[:, (2 * g + 1) * size : (2 * g + 2) * size]
        none, ones = jnp.zeros_like(keys), jnp.ones_like(values)
        wide = jnp.concatenate(
            [
                queries[here, (g * share + 2 * i) * size : (g * share + 2 * i + 2) * size]
                for i in range(pairs)
            ],
            0,
        )
        sides = []
        for odd in range(2):
            two_keys = jnp.concatenate([none, keys] if odd else [keys, none], 1)
            two_values = jnp.concatenate([ones, values] if odd else [values, ones], 1)
            score = dot(wide, two_keys, ((1,), (1,))) * size**-0.5
            score = jnp.where(allowed, score, -1e30)
            drain = jnp.concatenate(
                [
                    jnp.broadcast_to(
                        sink[0:1, g * share + 2 * i + odd : g * share + 2 * i + odd + 1],
                        (count, 1),
                    )
                    for i in range(pairs)
                ],
                0,
            )
            top = jnp.maximum(jnp.max(score, axis=1, keepdims=True), drain)
            grown = jnp.exp(score - top).astype(BF16)
            both = dot(grown, two_values)
            at = 0 if odd else size
            total = both[:, at : at + 1] + jnp.exp(drain - top)
            sides.append(both * (1.0 / total))
        lane = lax.broadcasted_iota(jnp.int32, (tall, 2 * size), 1)
        both = jnp.where(lane < size, sides[0], sides[1]).astype(BF16)
        for i in range(pairs):
            at = (g * share + 2 * i) * size
            attended[here, at : at + 2 * size] = both[i * count : (i + 1) * count]


def timeline(count, pieces, halves, favour=None):
    hop, narrow, tick = 0.7, 0.5, 0.05
    line_lead, layer_lead, begun, spare = 0.3, 0.6, 1.9, 0.3
    cost = {"close": 0.2, "pick": 0.07, "expert": 0.67, "mix": 0.08, "pass": 0.02}
    every = range(count)
    bits = [(s, p) for s in every for p in range(halves * pieces)]
    parts = [(s, q) for s in every for q in range(pieces)]
    landed, came, worked, back, mixed, handed = {}, {}, {}, {}, {}, {}
    line, layer, busy = {}, [1.1] * count, [begun] * count
    done = [set() for _ in every]
    steps = [[] for _ in every]
    now = 0.0

    def put(d, way, at, board, part, size):
        line[d, way] = max(line.get((d, way), 0.0), at) + size
        key = (d + way,) + part
        board[key] = max(board.get(key, 0.0), line[d, way] + hop)

    def there(board, d, part):
        return board.get((d,) + part, now + 1) <= now

    def whole(d, p):
        return all(there(landed, d, (p[0], h * pieces + p[1])) for h in range(halves))

    def choose(d):
        for way, name in ((-1, "send_out"), (1, "send_in")):
            if 0 <= d + way < count and line.get((d, way), 0.0) <= now + line_lead:
                ready = [
                    p
                    for p in bits
                    if (p[0] - d) * way <= 0 and there(landed, d, p) and (name, p) not in done[d]
                ]
                if ready:
                    end = d + way in (0, count - 1)
                    return name, min(ready, key=lambda p: (end and p[0] == d, abs(p[0] - d), p[1]))
        if ("close", (d, 0)) not in done[d]:
            return "close", (d, 0)
        ready = [
            p
            for p in parts
            if p[0] != d and there(handed, d, p) and there(mixed, d, p) and ("pass", p) not in done[d]
        ]
        if ready:
            return "pass", min(ready, key=lambda p: handed[(d,) + p])
        for p in parts:
            if there(back, d, p) and ("mix", p) not in done[d]:
                return "mix", p
        ready = [
            (s, 0)
            for s in every
            if there(came, d, (s, pieces - 1)) and ("expert", (s, 0)) not in done[d]
        ]
        if ready:
            return "expert", min(ready, key=lambda p: came[d, p[0], pieces - 1])
        ready = [p for p in parts if whole(d, p) and ("pick", p) not in done[d]]
        if ready and layer[d] <= now + layer_lead:
            return "pick", min(ready, key=lambda p: (favour[d][p[0]] if favour else 0, p))
        ready = [p for p in parts if p[0] == d and there(worked, d, p) and ("back", p) not in done[d]]
        ahead = [s for s in every if s != d and ("expert", (s, 0)) not in done[d]]
        if ready and layer[d] <= now and not ahead:
            return "back", ready[0]
        return None

    for d in every:
        for p in range(pieces):
            landed[d, d, p] = 0.0
            for way, name in ((-1, "send_out"), (1, "send_in")):
                if 0 <= d + way < count:
                    put(d, way, 0.0, landed, (d, p), 1 / halves)
                    done[d].add((name, (d, p)))
    size = count * pieces
    due = [{"mix": size, "pass": size - pieces if 0 < d < count - 1 else 0} for d in every]
    while any(sum(k == name for k, _ in done[d]) < due[d][name] for d in every for name in due[d]):
        for d in every:
            while busy[d] <= now:
                step = choose(d)
                if step is None:
                    break
                name, part = step
                done[d].add(step)
                steps[d].append((name,) + part)
                busy[d] = now + cost.get(name, 0.0)
                if name == "send_in":
                    put(d, 1, now, landed, part, 1 / halves)
                elif name == "send_out":
                    put(d, -1, now, landed, part, 1 / halves)
                elif name == "close":
                    for p in range(pieces, halves * pieces):
                        landed[d, d, p] = busy[d]
                elif name == "pick":
                    layer[d] = max(layer[d], busy[d]) + narrow
                    came[(d,) + part] = layer[d] + hop + (spare if 0 < d < count - 1 else 0)
                elif name == "expert":
                    for q in range(pieces):
                        if part[0] == d:
                            worked[d, d, q] = busy[d]
                            continue
                        ready = now + cost[name] * (q + 3) / (pieces + 2)
                        layer[d] = max(layer[d], ready) + narrow
                        back[d, part[0], q] = layer[d] + hop
                elif name == "back":
                    layer[d] = max(layer[d], now) + narrow
                    back[(d,) + part] = layer[d] + hop
                elif name == "mix":
                    mixed[(d,) + part] = busy[d]
                if name == "pass" or (name == "mix" and part[0] != d and d in (0, count - 1)):
                    put(d, 1 if part[0] > d else -1, busy[d], handed, part, 1)
        now += tick
    if favour is None:
        ends = [[landed[d, s, halves * pieces - 1] for s in every] for d in every]
        return timeline(count, pieces, halves, ends)
    return steps


def tail_kernel(
    sizes,
    queries_hbm, keys_hbm, values_hbm, sink_hbm, out_w_hbm, residual_hbm, gain_hbm, ids_hbm, weights_hbm,
    gate_hbm, up_hbm, down_hbm,
    out,
    queries, keys, values, sink, residual, gain, ids, weights, seen, attended, halo_send, halo_recv,
    out_w, gate_w, up_w, down_w,
    pair_out, pair_in, far_out, far_in, mine,
    stream, facts, slots, shares,
    tokens, outbox, arrived, results, returned,
    local, total_own, line_out, line_in,
    load_sem, pair_send, pair_recv, far_send, far_recv,
    facts_send, facts_recv, line_go_send, line_go_recv,
    go_send, go_recv, back_send, back_recv, line_back_send, line_back_recv,
):
    sp_count, tp_count, pieces, halves, capacity = sizes
    chips = tp_count // 2
    z, t = lax.axis_index("sp"), lax.axis_index("tp")
    x, core = t // 2, t % 2
    other = 1 - core
    rows, width = residual_hbm.shape
    piece, half = width // pieces, rows // halves
    top_k = ids_hbm.shape[0]
    picks = tp_count * capacity

    barrier = pltpu.get_barrier_semaphore()
    for k in range(1, sp_count):
        pl.semaphore_signal(
            barrier, inc=1, device_id={"sp": (z + k) % sp_count}, device_id_type=MESH
        )
    for k in range(1, tp_count):
        pl.semaphore_signal(
            barrier, inc=1, device_id={"tp": (t + k) % tp_count}, device_id_type=MESH
        )
    loads = [
        pltpu.make_async_copy(src, dst, load_sem.at[i])
        for i, (src, dst) in enumerate(
            (
                (keys_hbm, keys), (values_hbm, values), (queries_hbm, queries), (sink_hbm, sink),
                (ids_hbm, ids), (weights_hbm, weights), (out_w_hbm, out_w), (residual_hbm, residual),
                (gain_hbm, gain), (gate_hbm.at[0], gate_w), (up_hbm.at[0], up_w), (down_hbm.at[0], down_w),
            )
        )
    ]
    for load in loads:
        load.start()

    groups, size, reach = keys.shape
    for load in loads[:2]:
        load.wait()
    for g in range(groups):
        both = jnp.concatenate([keys[g], values[g]], 0)
        seen[WINDOW:, 2 * g * size : (2 * g + 2) * size] = both.T

    @pl.when(z == 0)
    def _():
        seen[:WINDOW, :] = jnp.zeros((WINDOW, seen.shape[1]), BF16)

    for load in loads[2:6]:
        load.wait()
    pad = jnp.zeros((-2 * top_k % 8, rows), F32)
    facts[z] = jnp.concatenate([ids[...].astype(F32), weights[...], pad], 0)
    def facts_copy(k):
        return pltpu.make_async_remote_copy(
            facts.at[z], facts.at[z], facts_send, facts_recv.at[z],
            device_id={"sp": (z + k) % sp_count}, device_id_type=MESH,
        )

    def facts_wait(s):
        pltpu.make_async_remote_copy(
            facts.at[s], facts.at[s], facts_send, facts_recv.at[s],
            device_id={"sp": s}, device_id_type=MESH,
        ).wait_recv()

    def route(s):
        slots[s], shares[s] = routing(facts[s], z * tp_count, top_k, tp_count, capacity)

    halo_copy = pltpu.make_async_remote_copy(
        seen.at[pl.ds(reach, WINDOW)], seen.at[pl.ds(0, WINDOW)], halo_send, halo_recv,
        device_id={"sp": jnp.minimum(z + 1, sp_count - 1)}, device_id_type=MESH,
    )

    def attend_half(at, h):
        attend(z, queries, sink, seen, attended, at * rows + h * half, half)

    def pair_copy(h, k, q):
        return pltpu.make_async_remote_copy(
            pair_out.at[h, k, q], pair_in.at[h, k, q], pair_send, pair_recv.at[h, k, q],
            device_id={"tp": x * 2 + other}, device_id_type=MESH,
        )

    def far_copy(h, q):
        return pltpu.make_async_remote_copy(
            far_out.at[h, q], far_in.at[h, q], far_send, far_recv.at[h, q],
            device_id={"tp": (1 - x) * 2 + core}, device_id_type=MESH,
        )

    def far_out_all(h):
        for q in range(pieces):
            pair_copy(h, 1, q).wait_recv()
            far_out[h, q] = (mine[h, 1, q] + pair_in[h, 1, q].astype(F32)).astype(BF16)
            far_copy(h, q).start()

    def taken(at, h):
        return attended[pl.ds(pl.multiple_of(at * rows + h * half, half), half), :]

    def give(h, k):
        chip = (x + k) % chips
        block = jnp.concatenate([taken(chip * 2 + other, h), taken(chip * 2 + core, h)], 0)
        for q in range(pieces):
            both = dot(block, out_w[:, q * piece : (q + 1) * piece])
            pair_out[h, k, q] = both[:half].astype(BF16)
            pair_copy(h, k, q).start()
            mine[h, k, q] = both[half:]
        if k:
            far_out_all(h)

    def give_one(h, at):
        block = taken(at, h)
        for q in range(pieces):
            one = dot(block, out_w[:, q * piece : (q + 1) * piece])

            @pl.when(at % 2 == core)
            def _():
                mine[h, 1, q] = one

            @pl.when(at % 2 == other)
            def _():
                pair_out[h, 1, q] = one.astype(BF16)
                pair_copy(h, 1, q).start()

        @pl.when(at % 2 == core)
        def _():
            far_out_all(h)

    def first_rows():
        @pl.when(z > 0)
        def _():
            halo_copy.wait_recv()

        attend_half(0, 0)

    def turn(h, k):
        chip = (x + k) % chips
        attend_half(chip * 2 + 1, h)
        attend_half(chip * 2, h)
        give(h, k)

    def close(h):
        here = slice(h * half, (h + 1) * half)
        square = jnp.zeros((half, 1), F32)
        for q in range(pieces):
            cols = slice(q * piece, (q + 1) * piece)
            total = mine[h, 0, q]
            pair_copy(h, 0, q).wait_recv()
            total = total + pair_in[h, 0, q].astype(F32)
            far_copy(h, q).wait_recv()
            total = total + far_in[h, q].astype(F32)
            value = (residual[here, cols].astype(F32) + total).astype(BF16)
            stream[here, cols] = value
            value = value.astype(F32)
            square = square + jnp.sum(value * value, axis=1, keepdims=True)
        scale = lax.rsqrt(square / width + EPS)
        for q in range(pieces):
            cols = slice(q * piece, (q + 1) * piece)
            tokens[z, q, here, :] = (stream[here, cols].astype(F32) * scale * gain[:, cols]).astype(BF16)

    def route_other(k, carry):
        s = (z + k) % sp_count
        facts_wait(s)
        route(s)
        return carry

    def line_go(to, s, p):
        bit = tokens.at[s, p % pieces, pl.ds(p // pieces * half, half)]
        return pltpu.make_async_remote_copy(
            bit, bit, line_go_send, line_go_recv.at[s, p],
            device_id={"sp": to}, device_id_type=MESH,
        )

    def line_back(to, s, q, way, last=False):
        return pltpu.make_async_remote_copy(
            line_out.at[s, q], line_in.at[way, s, q], line_back_send,
            line_back_recv.at[s + last * way * (sp_count - s), q], device_id={"sp": to}, device_id_type=MESH,
        )

    def go_copy(s, q, to, at):
        return pltpu.make_async_remote_copy(
            outbox.at[s, q, to], arrived.at[s, q, at], go_send, go_recv.at[s, q],
            device_id={"tp": to}, device_id_type=MESH,
        )

    def back_copy(s, q, to, at):
        return pltpu.make_async_remote_copy(
            results.at[s, q, to], returned.at[s, q, at], back_send, back_recv.at[s, q],
            device_id={"tp": to}, device_id_type=MESH,
        )

    def box_wait(box, send, recv, s, q):
        part = pl.ds(0, tp_count - 1)
        pltpu.make_async_remote_copy(
            box.at[s, q, part], box.at[s, q, part], send, recv.at[s, q],
            device_id={"tp": (t + 1) % tp_count}, device_id_type=MESH,
        ).wait_recv()

    def sent(ref, send, peer):
        pltpu.make_async_remote_copy(
            ref, ref, send, halo_recv, device_id=peer, device_id_type=MESH
        ).wait_send()

    peers = [(t + k) % tp_count for k in range(1, tp_count)]
    flip = (z * 2 >= sp_count).astype(jnp.int32)
    place = z + flip * (sp_count - 1 - 2 * z)

    def real(s):
        return s + flip * (sp_count - 1 - 2 * s)

    attend_half((chips - 1) * 2 + 1, 0)
    attend_half((chips - 1) * 2, 0)
    pl.semaphore_wait(barrier, sp_count + tp_count - 2)

    @pl.when(z < sp_count - 1)
    def _():
        halo_copy.start()

    for k in range(1, sp_count):
        facts_copy(k).start()
    loads[6].wait()

    @pl.when(x == 0)
    def _():
        give(0, 1)

    @pl.when(x == 1)
    def _():
        attend_half(1, 0)
        give_one(0, 1)
        first_rows()
        give_one(0, 0)

    turn(1, 1)

    @pl.when(x == 0)
    def _():
        attend_half(1, 0)
        first_rows()

    give(0, 0)
    for load in loads[7:9]:
        load.wait()
    close(0)
    for p in range(pieces):
        for way in (-1, 1):
            @pl.when((place + way >= 0) & (place + way < sp_count))
            def _():
                line_go(real(place + way), z, p).start()
    turn(1, 0)
    route(z)
    lax.fori_loop(1, sp_count, route_other, 0)

    def program(m):
        inner, outer = flip, 1 - flip

        def land(s, q):
            line_go(real(s), real(s), q).wait_recv()

        def send_in(s, q):
            line_go(real(m + 1), real(s), q).start()

        def send_out(s, q):
            line_go(real(m - 1), real(s), q).start()

        def pick(s, q):
            r = real(s)
            chosen = dot(slots[r], tokens[r, q]).astype(BF16)
            outbox[r, q] = chosen.reshape(tp_count, capacity, piece)
            for to in peers:
                go_copy(r, q, to, t).start()
            arrived[r, q, t] = outbox[r, q, t]

        def expert(s, _):
            r = real(s)
            gated = raised = None
            for q in range(pieces):
                box_wait(arrived, go_send, go_recv, r, q)
                block = arrived[r, q].reshape(picks, piece)
                part = slice(q * piece, (q + 1) * piece)
                a, b = dot(block, gate_w[part, :]), dot(block, up_w[part, :])
                gated, raised = (a, b) if q == 0 else (gated + a, raised + b)
            hidden = (gated / (1.0 + jnp.exp(-gated)) * raised).astype(BF16)
            for q in range(pieces):
                done = dot(hidden, down_w[:, q * piece : (q + 1) * piece]).astype(BF16)
                results[r, q] = done.reshape(tp_count, capacity, piece)
                if s != m:
                    give_back(s, q)
                returned[r, q, t] = results[r, q, t]

        def give_back(s, q):
            for to in peers:
                back_copy(real(s), q, to, t).start()

        def mix(s, q):
            r = real(s)
            box_wait(returned, back_send, back_recv, r, q)
            both = dot(shares[r], returned[r, q].reshape(picks, piece))
            mixed = both[:rows] + both[rows:]
            if s == m:
                total_own[q] = stream[:, q * piece : (q + 1) * piece].astype(F32) + mixed
            elif m == 0:
                line_out[r, q] = mixed.astype(BF16)
                line_back(real(1), r, q, inner, s == 1).start()
            else:
                local[r, q] = mixed

        def hand_on(s, q):
            r = real(s)
            way, to = (inner, m + 1) if s > m else (outer, m - 1)
            line_back(real(to), r, q, way).wait_recv()
            line_out[r, q] = (local[r, q] + line_in[way, r, q].astype(F32)).astype(BF16)
            line_back(real(to), r, q, way, s == to).start()

        act = {
            "close": lambda *_: close(1), "send_in": send_in, "send_out": send_out,
            "pick": pick, "expert": expert, "back": give_back, "mix": mix, "pass": hand_on,
        }
        waited = set()
        for name, s, q in steps[m]:
            if name == "expert" and "loads" not in waited:
                waited.add("loads")
                for load in loads[9:]:
                    load.wait()
            for p in range(q, halves * pieces, pieces) if name == "pick" else [q]:
                if name in ("pick", "send_in", "send_out") and s != m and (s, p) not in waited:
                    waited.add((s, p))
                    land(s, p)
            act[name](s, q)
        for q in range(pieces):
            total = total_own[q]
            for way in [inner, outer] if m > 0 else [outer]:
                line_back(real(m + 1), z, q, way, True).wait_recv()
                total = total + line_in[way, z, q].astype(F32)
            out[:, q * piece : (q + 1) * piece] = total.astype(BF16)
        peer = {"sp": real(m + 1)}
        for _ in range(sp_count + 1 if m > 0 else 1):
            sent(tokens.at[0], line_go_send, peer)
        sent(line_out.at[pl.ds(0, sp_count - 1)], line_back_send, peer)

    steps = timeline(sp_count, pieces, halves)
    for m in range((sp_count + 1) // 2):
        pl.when(place == m)(functools.partial(program, m))

    @pl.when(z < sp_count - 1)
    def _():
        halo_copy.wait_send()

    peer = {"tp": x * 2 + other}
    sent(facts.at[pl.ds(0, sp_count - 1)], facts_send, {"sp": (z + 1) % sp_count})
    sent(pair_out, pair_send, peer)
    sent(far_out, far_send, peer)
    sent(outbox.at[:, :, pl.ds(0, tp_count - 1)], go_send, peer)
    sent(results.at[:, :, pl.ds(0, tp_count - 1)], back_send, peer)


def fused(
    queries, key_heads, value_heads, sink_logit, out_weight, residual, norm_gain, expert_ids, route_weights,
    gate_weight, up_weight, down_weight,
):
    rows, width = residual.shape
    sp_count, tp_count = lax.axis_size("sp"), lax.axis_size("tp")
    experts = sp_count * tp_count
    top_k = expert_ids.shape[1]
    capacity = max(2, 2 * top_k * rows // experts)
    hidden = gate_weight.shape[2]
    depth = out_weight.shape[0]
    pieces, halves = 4, 2
    chips = tp_count // 2
    piece = width // pieces
    part = (halves, chips, pieces, rows // halves, piece)
    line = (sp_count, pieces, rows, piece)
    box = (sp_count, pieces, tp_count, capacity, piece)
    picks = tp_count * capacity
    reach, groups, size = key_heads.shape
    keys, values = key_heads.transpose(1, 2, 0), value_heads.transpose(1, 2, 0)
    vmem = pl.BlockSpec(memory_space=pltpu.VMEM)
    hbm = pl.BlockSpec(memory_space=pltpu.MemorySpace.HBM)
    dma = pltpu.SemaphoreType.DMA
    return pl.pallas_call(
        functools.partial(tail_kernel, (sp_count, tp_count, pieces, halves, capacity)),
        out_shape=pltpu.VMEM((rows, width), BF16),
        in_specs=[hbm] * 12,
        out_specs=vmem,
        scratch_shapes=[
            pltpu.VMEM(queries.shape, BF16),
            pltpu.VMEM(keys.shape, BF16),
            pltpu.VMEM(values.shape, BF16),
            pltpu.VMEM((1,) + sink_logit.shape, F32),
            pltpu.VMEM(residual.shape, BF16),
            pltpu.VMEM((1,) + norm_gain.shape, F32),
            pltpu.VMEM((top_k, rows), jnp.int32),
            pltpu.VMEM((top_k, rows), F32),
            pltpu.VMEM((WINDOW + reach, groups * 2 * size), BF16),
            pltpu.VMEM(queries.shape, BF16),
            dma,
            dma,
            pltpu.VMEM((depth, width), BF16),
            pltpu.VMEM((width, hidden), BF16),
            pltpu.VMEM((width, hidden), BF16),
            pltpu.VMEM((hidden, width), BF16),
            pltpu.VMEM(part, BF16),
            pltpu.VMEM(part, BF16),
            pltpu.VMEM(part[:1] + part[2:], BF16),
            pltpu.VMEM(part[:1] + part[2:], BF16),
            pltpu.VMEM(part, F32),
            pltpu.VMEM((rows, width), BF16),
            pltpu.VMEM((sp_count, 2 * top_k + -2 * top_k % 8, rows), F32),
            pltpu.VMEM((sp_count, picks, rows), BF16),
            pltpu.VMEM((sp_count, 2 * rows, picks), BF16),
            pltpu.VMEM(line, BF16),
            pltpu.VMEM(box, BF16),
            pltpu.VMEM(box, BF16),
            pltpu.VMEM(box, BF16),
            pltpu.VMEM(box, BF16),
            pltpu.VMEM(line, F32),
            pltpu.VMEM(line[1:], F32),
            pltpu.VMEM(line, BF16),
            pltpu.VMEM((2,) + line, BF16),
            dma((12,)),
            dma,
            dma((halves, chips, pieces)),
            dma,
            dma((halves, pieces)),
            dma,
            dma((sp_count,)),
            dma,
            dma((sp_count, halves * pieces)),
            dma,
            dma((sp_count, pieces)),
            dma,
            dma((sp_count, pieces)),
            dma,
            dma((sp_count + 1, pieces)),
        ],
        compiler_params=pltpu.CompilerParams(
            collective_id=0, has_side_effects=True, vmem_limit_bytes=VMEM_BUDGET
        ),
    )(
        queries, keys, values, sink_logit[None], out_weight, residual, norm_gain[None], expert_ids.T, route_weights.T,
        gate_weight, up_weight, down_weight,
    )


def on_device(queries, key_heads, value_heads, sink_logit, *rest):
    rows_dev = rest[1].shape[0]
    experts = lax.axis_size("sp") * lax.axis_size("tp")
    fits = 2 * rest[3].shape[1] * rows_dev // experts % 16 == 0 and rows_dev % WINDOW == 0
    fits = fits and lax.axis_size("sp") > 1 and lax.axis_size("tp") == 4
    if fits:
        return fused(queries, key_heads, value_heads, sink_logit, *rest)
    return tail_plain(attention(queries, key_heads, value_heads, sink_logit), *rest)


def solution(mesh):
    return jax.shard_map(
        on_device,
        mesh=mesh,
        in_specs=(
            P(("grp", "sp"), "tp"),
            P(("grp", "sp"), "tp", None),
            P(("grp", "sp"), "tp", None),
            P("tp"),
            P("tp", None),
            P(("grp", "sp", "tp"), None),
            P(),
            P(("grp", "sp", "tp"), None),
            P(("grp", "sp", "tp"), None),
            P(("sp", "tp"), None, None),
            P(("sp", "tp"), None, None),
            P(("sp", "tp"), None, None),
        ),
        out_specs=P(("grp", "sp", "tp"), None),
        check_vma=False,
    )
```
